256 devices in a mesh: sp: 64 (over z, y, core), tp: 4 (over x).
Axes of the slice: x: 4, y: 4, z: 8, core: 2. Of those that a mesh axis runs over, the one named last changes fastest.
Arguments:
- cotangent: bfloat16 [16384, 2048], P('sp'), may hold values from -16 to 16
- stream_in: bfloat16 [16384, 2048], P('sp'), may hold values from -6 to 6
- norm_gain: float32 [2048], replicated, may hold values from 0.1 to 1.9
- out_gate: bfloat16 [16384, 1024], P('sp', 'tp'), may hold values from -6 to 6
- in_gate: bfloat16 [16384, 1024], P('sp', 'tp'), may hold values from -6 to 6
- conv_input: bfloat16 [16384, 1024], P('sp', 'tp'), may hold values from -6 to 6
- conv_taps: float32 [3, 1024], P(None, 'tp'), may hold values from -3 to 3
- out_weight: bfloat16 [2048, 1024], P(None, 'tp'), may hold values from -0.1875 to 0.1875
- expert_gate: bfloat16 [64, 2048, 1024], P('sp', None, 'tp'), may hold values from -0.125 to 0.125
- expert_up: bfloat16 [64, 2048, 1024], P('sp', None, 'tp'), may hold values from -0.125 to 0.125
- expert_down: bfloat16 [64, 1024, 2048], P('sp', 'tp'), may hold values from -0.1875 to 0.1875
- expert_choice: int32 [16384, 2], P('sp'), may hold values from 0 to 63, all different within a row; in each aligned block of 256 rows (0 to 255, 256 to 511, ...) at most 16 rows name the same one
- route_scale: float32 [16384, 2], P('sp'), may hold values from 0.05 to 0.6
Outputs:
- grad_stream: bfloat16 [16384, 2048], P('sp', 'tp')
- grad_out_gate: bfloat16 [16384, 1024], P('sp', 'tp')
- grad_in_gate: bfloat16 [16384, 1024], P('sp', 'tp')
- grad_conv_input: bfloat16 [16384, 1024], P('sp', 'tp')
- grad_out_weight: float32 [2048, 1024], P('sp', 'tp')
- grad_expert_gate: float32 [64, 2048, 1024], P('sp', None, 'tp')
- grad_expert_up: float32 [64, 2048, 1024], P('sp', None, 'tp')
- grad_expert_down: float32 [64, 1024, 2048], P('sp', 'tp')
The draws below stay inside these ranges and needn't reach their ends.
Inputs may be any that keep to these rules, and one draw needn't show every extreme that they name: `expert_choice`: each row names two different experts. Within the rows of one device no expert is named more than 16 times, a bound that some block reaches in some devices' rows.
All inputs are finite; a program needn't handle non-finite values.
Results may differ from the reference program's by a relative error of at most 0.01.
Values may be sent and summed in bfloat16 or wider, within the bound.
A program may use at most 128 MiB of HBM per device.

```python
import math
import jax
import jax.numpy as jnp
import numpy as np
from jax import lax

D = 2048
CW = 1024
FF = 1024
TAPS = 3
TOK_DEV = 256
TOKENS = 16384
EXPERTS = 64
CAP = 16
N_SP = 64
N_TP = 4


def raised(drawn, rng, source, target, shards_of, factor):
    def block_of(dim):
        return (jnp.arange(drawn.shape[dim]) // (drawn.shape[dim] // shards_of)).reshape((-1,) + (1,) * (drawn.ndim - 1 - dim))

    first = jax.random.permutation(rng, shards_of)[block_of(target)]
    other_side = (block_of(target) + shards_of // 2) % shards_of
    return jnp.where((block_of(source) == first) | (block_of(source) == other_side), factor * drawn, drawn)


def shard_levels(rng, dims, cuts, low, top_value):
    def one(axis_at, blocks):
        heights = jax.random.uniform(jax.random.fold_in(jax.random.fold_in(rng, 6), axis_at), (blocks,), jnp.float32, low / len(cuts), top_value / len(cuts))
        return jnp.repeat(jnp.exp(heights), dims[axis_at] // blocks).reshape((-1,) + (1,) * (len(dims) - axis_at - 1))

    factor_of = one(*cuts[0])
    for cut in cuts[1:]:
        factor_of = factor_of * one(*cut)
    return factor_of


def deal_out(key, own, number, rows, count, top, reach, slope):
    sequence = jax.random.permutation(key, count)
    heavy_load, common = load_shares(count, rows * top, reach, slope, True), load_shares(count, rows * top, reach, slope, False)
    places = jnp.arange(count)

    def named(lengths, offset_by):
        used = int((lengths > 0).sum())
        fixed = max(1, used // 4)
        passed = fixed + (places - fixed + offset_by * (used - fixed)) % max(1, count - fixed)
        return jnp.zeros((count,), jnp.int32).at[sequence[jnp.where(places < fixed, places, passed)]].set(jnp.asarray(lengths, jnp.int32))

    lengths = jnp.where(number % 4 == 0, named(heavy_load, number // 4), named(common, number - number // 4 - 1))
    mixed = jax.random.permutation(jax.random.fold_in(own, 3), count)
    source_of, sink = mixed[0:count // 2 * 2:2], mixed[1:count // 2 * 2:2]
    slack = jnp.minimum(lengths[source_of] - 1, reach - lengths[sink]) // 2
    slack = jnp.where((source_of == sequence[0]) | (sink == sequence[0]) | (lengths[sink] == 0), 0, jnp.maximum(slack, 0))
    passed = jax.random.randint(jax.random.fold_in(own, 4), (count // 2,), 0, 1 << 20) % (slack + 1)
    lengths = lengths.at[source_of].add(-passed).at[sink].add(passed)
    members = jnp.searchsorted(jnp.cumsum(lengths), jnp.arange(rows * top), side="right").astype(jnp.int32)
    grid = members.reshape(top, rows).T
    grid = grid[jax.random.permutation(jax.random.fold_in(own, 1), rows)]
    offset_by = jax.random.randint(jax.random.fold_in(own, 2), (rows, 1), 0, top)
    return jnp.take_along_axis(grid, (jnp.arange(top)[None, :] + offset_by) % top, axis=1)


def load_shares(number_of, total, most, slope, full):
    loads = [(1 << 20) // math.isqrt(standing ** slope) + 1 for standing in range(1, number_of + 1)]
    largest = most if full else min(most, max(-(-total // number_of), total * loads[0] // sum(loads)))
    least = 1 if total - largest >= number_of - 1 else 0
    holding, surplus = [largest] + [least] * (number_of - 1), total - largest - least * (number_of - 1)
    while surplus > 0:
        free = [i for i in range(1, number_of) if holding[i] < largest] or [i for i in range(1, number_of) if holding[i] < most]
        pool, left = sum([loads[i] for i in free]), surplus
        for i in free:
            more = min(most - holding[i], max(1, left * loads[i] // pool), surplus)
            holding[i] = holding[i] + more
            surplus = surplus - more
    return np.array(holding)


def normal_values(rng, shape, spread, reach, cuts=(), kind=jnp.bfloat16):
    array = spread * jax.random.normal(rng, shape, jnp.float32)
    if cuts:
        array = array * shard_levels(rng, shape, cuts, -0.22, 0.18)
    return jnp.clip(array, -reach, reach).astype(kind)


def gaussian_with(own_key, extent, width, most, pieces, heavy, kind=jnp.bfloat16):
    values = width * jax.random.normal(own_key, extent, jnp.float32)
    if pieces:
        values = values * shard_levels(own_key, extent, pieces, -0.22, 0.18)
    return jnp.clip(raised(values, jax.random.fold_in(own_key, 3), *heavy), -most, most).astype(kind)


def setup_inputs(seed: int = 0) -> dict:
    streams_of = jax.random.split(jax.random.key(seed), 14)
    cotangent = gaussian_with(streams_of[0], (TOKENS, D), 1.0, 16.0, ((0, 64),), (0, 1, 64, 4.0))
    stream_in = normal_values(streams_of[1], (TOKENS, D), 1.0, 6.0, ((0, 64),))
    norm_gain = jnp.clip(1.0 + 0.18 * jax.random.normal(streams_of[2], (D,), jnp.float32), 0.1, 1.9)
    out_gate = normal_values(streams_of[3], (TOKENS, CW), 1.0, 6.0, ((0, 64), (1, 4)))
    in_gate = normal_values(streams_of[4], (TOKENS, CW), 1.0, 6.0, ((0, 64), (1, 4)))
    conv_input = normal_values(streams_of[5], (TOKENS, CW), 1.0, 6.0, ((0, 64), (1, 4)))
    conv_taps = normal_values(streams_of[6], (TAPS, CW), 0.577, 3.0, ((1, 4),), jnp.float32)
    out_weight = normal_values(streams_of[7], (D, CW), CW ** -0.5, 0.1875, ((1, 4),))
    expert_gate = normal_values(streams_of[8], (EXPERTS, D, FF), D ** -0.5, 0.125, ((0, 64), (2, 4)))
    expert_up = normal_values(streams_of[9], (EXPERTS, D, FF), D ** -0.5, 0.125, ((0, 64), (2, 4)))
    expert_down = normal_values(streams_of[10], (EXPERTS, FF, D), FF ** -0.5, 0.1875, ((0, 64), (1, 4)))
    expert_choice_keys = jax.random.split(jax.random.fold_in(streams_of[11], 1), TOKENS // TOK_DEV)
    expert_choice_turns = jax.random.permutation(jax.random.fold_in(streams_of[11], 3), TOKENS // TOK_DEV)
    expert_choice = jax.vmap(lambda own, number: deal_out(jax.random.fold_in(streams_of[11], 2), own, number, TOK_DEV, EXPERTS, 2, CAP, 2))(expert_choice_keys, expert_choice_turns).reshape((TOKENS, 2))
    route_scale = jnp.clip(0.05 + 0.55 * jax.random.uniform(streams_of[12], (TOKENS, 2), jnp.float32) ** shard_levels(streams_of[12], (TOKENS, 2), ((0, 64),), -0.2, 0.2), 0.05, 0.6)
    return {"cotangent": cotangent, "stream_in": stream_in, "norm_gain": norm_gain, "out_gate": out_gate, "in_gate": in_gate, "conv_input": conv_input, "conv_taps": conv_taps, "out_weight": out_weight, "expert_gate": expert_gate, "expert_up": expert_up, "expert_down": expert_down, "expert_choice": expert_choice, "route_scale": route_scale}


norm_eps = 1e-06

def slot_table(choice_rows, expert_count, capacity):
    flat_ids = choice_rows.reshape(-1).astype(jnp.int32)
    route_count = flat_ids.shape[0]
    onehot = (flat_ids[:, None] == jnp.arange(expert_count, dtype=jnp.int32)[None, :]).astype(jnp.int32)
    earlier = jnp.cumsum(onehot, axis=0) - onehot
    position = lax.optimization_barrier(jnp.sum(earlier * onehot, axis=1)).astype(jnp.int32)
    slot_of_route = (flat_ids * capacity + position).astype(jnp.int32)
    route_of_slot = jnp.full((expert_count * capacity,), route_count, jnp.int32)
    route_of_slot = route_of_slot.at[slot_of_route].set(jnp.arange(route_count, dtype=jnp.int32))
    return (slot_of_route, route_of_slot)

def rows_product(left, right):
    return lax.dot_general(left, right, (((0,), (0,)), ((), ())), preferred_element_type=jnp.float32)

def cols_product(left, right):
    return lax.dot_general(left, right, (((1,), (1,)), ((), ())), preferred_element_type=jnp.float32)

def reference(cotangent, stream_in, norm_gain, out_gate, in_gate, conv_input, conv_taps, out_weight, expert_gate, expert_up, expert_down, expert_choice, route_scale):
    stream = stream_in.astype(jnp.float32)
    inverse_rms = lax.rsqrt(lax.optimization_barrier(jnp.mean(stream * stream, axis=-1, keepdims=True)) + norm_eps)
    unit_stream = stream * inverse_rms
    normed = (unit_stream * norm_gain.astype(jnp.float32)).astype(jnp.bfloat16)
    capacity = 4 * TOK_DEV // N_SP
    route_count = 2 * TOK_DEV
    block_ids = expert_choice.reshape(N_SP, TOK_DEV, 2)
    tables = jax.vmap(lambda choice_block: slot_table(choice_block, EXPERTS, capacity)[1])(block_ids)
    flat_scale = route_scale.reshape(-1)
    source_base = (jnp.arange(N_SP, dtype=jnp.int32) * route_count)[:, None]
    width_tp = FF // N_TP

    def expert_step(accum, inputs):
        w_gate, w_up, w_down, expert = inputs
        chosen = lax.dynamic_slice_in_dim(tables, (expert * capacity).astype(jnp.int32), capacity, 1)
        present = chosen < route_count
        routes = (source_base + jnp.where(present, chosen, 0)).reshape(-1).astype(jnp.int32)
        present = present.reshape(-1)
        token = (routes // 2).astype(jnp.int32)
        weight = jnp.where(present, flat_scale[routes], jnp.zeros((), jnp.float32))
        scaled_cot = (cotangent[token].astype(jnp.float32) * weight[:, None]).astype(jnp.bfloat16)
        expert_rows = jnp.where(present[:, None], normed[token], jnp.zeros((), jnp.bfloat16))
        gate_pre = jnp.dot(expert_rows, w_gate, preferred_element_type=jnp.float32)
        up_pre = jnp.dot(expert_rows, w_up, preferred_element_type=jnp.float32)
        sigmoid_gate = jax.nn.sigmoid(gate_pre)
        silu_gate = gate_pre * sigmoid_gate
        hidden = (silu_gate * up_pre).astype(jnp.bfloat16)
        grad_down = rows_product(hidden, scaled_cot)
        hidden_grad = cols_product(scaled_cot, w_down)
        gate_grad = (hidden_grad * up_pre * sigmoid_gate * (1.0 + gate_pre * (1.0 - sigmoid_gate))).astype(jnp.bfloat16)
        up_grad = (hidden_grad * silu_gate).astype(jnp.bfloat16)
        grad_gate = rows_product(expert_rows, gate_grad)
        grad_up = rows_product(expert_rows, up_grad)
        slot_rows = expert_rows.shape[0]
        shares = jnp.einsum('rpf,dpf->prd', gate_grad.astype(jnp.float32).reshape(slot_rows, N_TP, width_tp), w_gate.astype(jnp.float32).reshape(D, N_TP, width_tp))
        shares = shares + jnp.einsum('rpf,dpf->prd', up_grad.astype(jnp.float32).reshape(slot_rows, N_TP, width_tp), w_up.astype(jnp.float32).reshape(D, N_TP, width_tp))
        rounded = lax.optimization_barrier(shares.astype(jnp.bfloat16))
        slot_grad = lax.optimization_barrier(jnp.sum(rounded.astype(jnp.float32), axis=0)).astype(jnp.bfloat16)
        slot_grad = lax.optimization_barrier(slot_grad)
        accum = accum.at[token].add(jnp.where(present[:, None], slot_grad.astype(jnp.float32), jnp.zeros((), jnp.float32)))
        return (accum, (grad_gate, grad_up, grad_down))
    start_accum = jnp.zeros((TOKENS, D), jnp.float32)
    accum, grads = lax.scan(expert_step, start_accum, (expert_gate, expert_up, expert_down, jnp.arange(EXPERTS, dtype=jnp.int32)))
    grad_gate, grad_up, grad_down = grads
    token_grad = lax.optimization_barrier(accum.astype(jnp.bfloat16))
    unit_grad = token_grad.astype(jnp.float32) * norm_gain.astype(jnp.float32)
    along = lax.optimization_barrier(jnp.mean(unit_stream * unit_grad, axis=-1, keepdims=True))
    stream_grad = (cotangent.astype(jnp.float32) + inverse_rms * (unit_grad - unit_stream * along)).astype(jnp.bfloat16)
    taps = conv_taps.astype(jnp.float32)
    product = in_gate.astype(jnp.float32) * conv_input.astype(jnp.float32)
    padded = jnp.pad(product, ((2, 0), (0, 0)))
    filtered = taps[0] * product + taps[1] * padded[1:-1] + taps[2] * padded[:-2]
    mixed_in = (out_gate.astype(jnp.float32) * filtered).astype(jnp.bfloat16)
    mixed_grad = jnp.dot(stream_grad, out_weight, preferred_element_type=jnp.float32)
    grad_out_gate = (mixed_grad * filtered).astype(jnp.bfloat16)
    filtered_grad = mixed_grad * out_gate.astype(jnp.float32)
    padded_grad = jnp.pad(filtered_grad, ((0, 2), (0, 0)))
    product_grad = taps[0] * filtered_grad + taps[1] * padded_grad[1:-1] + taps[2] * padded_grad[2:]
    grad_in_gate = (product_grad * conv_input.astype(jnp.float32)).astype(jnp.bfloat16)
    grad_conv_input = (product_grad * in_gate.astype(jnp.float32)).astype(jnp.bfloat16)
    grad_out_weight = rows_product(stream_grad, mixed_in)
    return (stream_grad, grad_out_gate, grad_in_gate, grad_conv_input, grad_out_weight, grad_gate, grad_up, grad_down)
```

```python
import functools

import jax
import jax.numpy as jnp
from jax import lax
from jax.experimental import pallas as pl
from jax.experimental.pallas import tpu as pltpu
from jax.sharding import PartitionSpec as P

norm_eps = 1e-06
MESH = pl.DeviceIdType.MESH
CAP = 16
BF = jnp.bfloat16
F32 = jnp.float32


def split_up(array, dim, peers):
    dims = array.shape
    tiles = array.reshape(*dims[:dim], peers, dims[dim] // peers, *dims[dim + 1 :])
    return jnp.moveaxis(tiles, dim, 0)


def sent_and_summed(array, axis, dim):
    tiles = split_up(array, dim, lax.axis_size(axis))
    arrived = lax.all_to_all(tiles, axis, split_axis=0, concat_axis=0, tiled=True)
    return arrived.astype(jnp.float32).sum(axis=0)


def passed_along(value, axis, steps):
    count = lax.axis_size(axis)
    first, last = (max(0, -steps), min(count, count - steps))
    return lax.ppermute(value, axis, [(source, source + steps) for source in range(first, last)])


def rows_product(left, right):
    return lax.dot_general(left, right, (((0,), (0,)), ((), ())), preferred_element_type=F32)


def cols_product(left, right):
    return lax.dot_general(left, right, (((1,), (1,)), ((), ())), preferred_element_type=F32)


def product_of(left, right):
    return jnp.dot(left, right, preferred_element_type=F32)


def loop(low, high, body):
    def step(i, carry):
        body(i)
        return carry

    lax.fori_loop(low, high, step, 0)


def offset_of(t):
    return lax.rem(t + lax.div(t + 7, 8), 8) + lax.div(t, 7)


def expert_kernel(
    plane, choice, scale, cot, stream, gain, wg, wu, wd,
    tok, out_gate, out_up, out_down,
    normed, pick, weight, send_all, send_part, rows, partial, summand, total, back, hidden, ggrad, ugrad,
    a_send, a_recv, right_send, left_send, from_left, from_right,
    fright_send, fleft_send, ffrom_left, ffrom_right,
    rs_send, rs_recv, ret_send, ret_recv, tok_send, tok_recv,
):
    me = lax.axis_index("sp")
    q = lax.axis_index("tp")
    right = lax.rem(q + 1, 4)
    left = lax.rem(q + 3, 4)
    z = lax.div(me, plane)
    place = lax.rem(me, plane)
    experts = 8 * plane
    span = plane * CAP
    tokens, width = cot.shape
    part = width // 4
    mine = pl.ds(pl.multiple_of(q * part, part), part)
    my_slots = pl.ds(pl.multiple_of(me * CAP, CAP), CAP)

    def span_of(plane_at):
        return pl.ds(pl.multiple_of(plane_at * span, span), span)

    def wait_for(ref, sem):
        pltpu.make_async_copy(ref, ref, sem).wait()

    barrier = pltpu.get_barrier_semaphore()

    def greet(k):
        pl.semaphore_signal(barrier, inc=1, device_id=(lax.rem(me + k, experts), q), device_id_type=MESH)

    loop(1, experts, greet)

    def greet_row(k):
        pl.semaphore_signal(barrier, inc=1, device_id=(me, lax.rem(q + k, 4)), device_id_type=MESH)

    loop(1, 4, greet_row)

    x = stream[...].astype(F32)
    inverse = lax.rsqrt(jnp.mean(x * x, axis=-1, keepdims=True) + norm_eps)
    normed[...] = ((x * inverse) * gain[...]).astype(BF)

    first, second = choice[0:1, :], choice[1:2, :]
    ids = lax.broadcasted_iota(jnp.int32, (experts, tokens), 0)
    is_first, is_second = ids == first, ids == second
    named = jnp.where(is_first | is_second, 1.0, 0.0).astype(BF)
    before = jnp.where(
        lax.broadcasted_iota(jnp.int32, (tokens, tokens), 0) < lax.broadcasted_iota(jnp.int32, (tokens, tokens), 1), 1.0, 0.0
    ).astype(BF)
    earlier = product_of(named, before)
    slot_first = first * CAP + jnp.sum(jnp.where(is_first, earlier, 0.0), axis=0, keepdims=True).astype(jnp.int32)
    slot_second = second * CAP + jnp.sum(jnp.where(is_second, earlier, 0.0), axis=0, keepdims=True).astype(jnp.int32)
    slots = lax.broadcasted_iota(jnp.int32, (experts * CAP, tokens), 0)
    at_first, at_second = slots == slot_first, slots == slot_second
    pick[...] = jnp.where(at_first | at_second, 1.0, 0.0).astype(BF)
    weight[...] = jnp.sum(
        jnp.where(at_first, scale[0:1, :], 0.0) + jnp.where(at_second, scale[1:2, :], 0.0), axis=1, keepdims=True
    )

    pl.semaphore_wait(barrier, experts + 2)

    def send_quarter(t):
        target = lax.rem(z + offset_of(t), 8)
        chosen = pick[span_of(target), :]
        send_part[t - 1, 0] = product_of(chosen, normed[:, mine]).astype(BF)
        send_part[t - 1, 1] = (product_of(chosen, cot[:, mine]) * weight[span_of(target), :]).astype(BF)

        def one(k):
            block = pl.ds(pl.multiple_of(k * CAP, CAP), CAP)
            pltpu.make_async_remote_copy(
                send_part.at[t - 1, :, block, :], rows.at[:, my_slots, mine], a_send.at[t], a_recv.at[t],
                device_id=(target * plane + k, q), device_id_type=MESH,
            ).start()

        loop(0, plane, one)

    loop(1, 6, send_quarter)

    def send_whole(i):
        t = i + 5 * lax.div(i + 1, 2)
        target = lax.rem(z + offset_of(t), 8)
        chosen = pick[span_of(target), :]
        send_all[i, 0] = product_of(chosen, normed[...]).astype(BF)
        send_all[i, 1] = (product_of(chosen, cot[...]) * weight[span_of(target), :]).astype(BF)

        def one(k):
            block = pl.ds(pl.multiple_of(k * CAP, CAP), CAP)

            @pl.when(target * plane + k != me)
            def _():
                pltpu.make_async_remote_copy(
                    send_all.at[i, :, block, :], rows.at[:, my_slots, :], a_send.at[t], a_recv.at[t],
                    device_id=(target * plane + k, q), device_id_type=MESH,
                ).start()

        loop(0, plane, one)

    loop(0, 3, send_whole)
    own = pl.ds(pl.multiple_of(place * CAP, CAP), CAP)
    rows[0, my_slots, :] = send_all[0, 0, own, :]
    rows[1, my_slots, :] = send_all[0, 1, own, :]

    def step(i):
        @pl.when((i >= 1) & (i < 6))
        def _():
            at = span_of(lax.rem(z + 8 - offset_of(i), 8))
            piece = rows.at[:, at, mine]
            wait_for(piece, a_recv.at[i])
            pltpu.make_async_remote_copy(
                piece, piece, right_send.at[i], from_left.at[i], device_id=(me, right), device_id_type=MESH
            ).start()
            pltpu.make_async_remote_copy(
                piece, piece, left_send.at[i], from_right.at[i], device_id=(me, left), device_id_type=MESH
            ).start()

        @pl.when((i >= 2) & (i < 7))
        def _():
            t = i - 1
            at = span_of(lax.rem(z + 8 - offset_of(t), 8))
            of_left = rows.at[:, at, pl.ds(pl.multiple_of(left * part, part), part)]
            of_right = rows.at[:, at, pl.ds(pl.multiple_of(right * part, part), part)]
            wait_for(of_left, from_left.at[t])
            half = rows.at[0, at, pl.ds(pl.multiple_of(left * part, part), part)]
            pltpu.make_async_remote_copy(
                half, half, fright_send.at[t], ffrom_left.at[t], device_id=(me, right), device_id_type=MESH
            ).start()
            wait_for(of_right, from_right.at[t])
            half = rows.at[1, at, pl.ds(pl.multiple_of(right * part, part), part)]
            pltpu.make_async_remote_copy(
                half, half, fleft_send.at[t], ffrom_right.at[t], device_id=(me, left), device_id_type=MESH
            ).start()

        @pl.when((i >= 2) & (i < 10))
        def _():
            t = i - 2
            at = span_of(lax.rem(z + 8 - offset_of(t), 8))

            @pl.when((t >= 1) & (t < 6))
            def _():
                far = pl.ds(pl.multiple_of(lax.rem(q + 2, 4) * part, part), part)
                wait_for(rows.at[0, at, far], ffrom_left.at[t])
                wait_for(rows.at[1, at, far], ffrom_right.at[t])

            @pl.when(t == 0)
            def _():
                others = rows.at[:, pl.ds(0, (plane - 1) * CAP), :]
                if plane > 1:
                    wait_for(others, a_recv.at[0])

            @pl.when(t >= 6)
            def _():
                wait_for(rows.at[:, at, :], a_recv.at[t])

            here = rows[0, at, :]
            gate_pre = product_of(here, wg[...])
            up_pre = product_of(here, wu[...])
            hidden_grad = cols_product(rows[1, at, :], wd[...])
            sigmoid_gate = jax.nn.sigmoid(gate_pre)
            silu_gate = gate_pre * sigmoid_gate
            hidden[at, :] = (silu_gate * up_pre).astype(BF)
            gate_grad = (hidden_grad * up_pre * sigmoid_gate * (1.0 + gate_pre * (1.0 - sigmoid_gate))).astype(BF)
            up_grad = (hidden_grad * silu_gate).astype(BF)
            ggrad[at, :] = gate_grad
            ugrad[at, :] = up_grad
            partial[at, :] = (cols_product(gate_grad, wg[...]) + cols_product(up_grad, wu[...])).astype(BF)

            def one(d):
                to = lax.rem(q + d, 4)
                pltpu.make_async_remote_copy(
                    partial.at[at, pl.ds(pl.multiple_of(to * part, part), part)], summand.at[d - 1, at, :],
                    rs_send.at[t], rs_recv.at[t], device_id=(me, to), device_id_type=MESH,
                ).start()

            loop(1, 4, one)

        @pl.when(i >= 4)
        def _():
            t = i - 4
            source = lax.rem(z + 8 - offset_of(t), 8)
            at = span_of(source)
            wait_for(summand.at[:, at, :], rs_recv.at[t])
            added = partial[at, mine].astype(F32)
            for d in range(3):
                added = added + summand[d, at, :].astype(F32)
            total[at, :] = added.astype(BF)

            def one(k):
                block = pl.ds(pl.multiple_of(source * span + k * CAP, CAP), CAP)

                @pl.when(source * plane + k != me)
                def _():
                    pltpu.make_async_remote_copy(
                        total.at[block, :], back.at[my_slots, :], ret_send, ret_recv,
                        device_id=(source * plane + k, q), device_id_type=MESH,
                    ).start()

            loop(0, plane, one)

    loop(0, 12, step)
    back[my_slots, :] = total[my_slots, :]

    chunk = min(256, width)

    def grads(m):
        cols = pl.ds(pl.multiple_of(m * chunk, chunk), chunk)
        here = rows[0, :, cols]
        out_gate[cols, :] = rows_product(here, ggrad[...])
        out_up[cols, :] = rows_product(here, ugrad[...])
        out_down[:, cols] = rows_product(hidden[...], rows[1, :, cols])

    loop(0, width // chunk, grads)

    wait_for(back.at[pl.ds(0, (experts - 1) * CAP), :], ret_recv)
    tok[:, mine] = rows_product(pick[...], back[...]).astype(BF)

    def share(d):
        pltpu.make_async_remote_copy(
            tok.at[:, mine], tok.at[:, mine], tok_send, tok_recv.at[d - 1],
            device_id=(me, lax.rem(q + d, 4)), device_id_type=MESH,
        ).start()

    loop(1, 4, share)

    def sent_rows(t):
        @pl.when((t >= 1) & (t < 6))
        def _():
            at = span_of(lax.rem(z + 8 - offset_of(t), 8))
            piece = rows.at[:, at, mine]
            wait_for(piece, a_send.at[t])
            wait_for(piece, right_send.at[t])
            wait_for(piece, left_send.at[t])
            wait_for(rows.at[0, at, mine], fright_send.at[t])
            wait_for(rows.at[0, at, mine], fleft_send.at[t])

        @pl.when(t == 0)
        def _():
            if plane > 1:
                wait_for(rows.at[:, pl.ds(0, (plane - 1) * CAP), :], a_send.at[0])

        @pl.when(t >= 6)
        def _():
            wait_for(rows.at[:, span_of(0), :], a_send.at[t])

        wait_for(summand.at[:, span_of(0), :], rs_send.at[t])

    loop(0, 8, sent_rows)
    wait_for(back.at[pl.ds(0, (experts - 1) * CAP), :], ret_send)

    def shared(d):
        wait_for(tok.at[:, mine], tok_recv.at[d])

    loop(0, 3, shared)
    wait_for(tok.at[:, pl.ds(0, 3 * part)], tok_send)


def through_experts(choice, scale, cot, stream, gain, wg, wu, wd, experts):
    tokens, width = cot.shape
    part = width // 4
    slots = experts * CAP
    plane = experts // 8
    hid = wg.shape[1]
    vm = pl.BlockSpec(memory_space=pltpu.VMEM)
    dma8 = pltpu.SemaphoreType.DMA((8,))
    return pl.pallas_call(
        functools.partial(expert_kernel, plane),
        name="experts",
        out_shape=(
            jax.ShapeDtypeStruct((tokens, width), BF),
            jax.ShapeDtypeStruct((width, hid), F32),
            jax.ShapeDtypeStruct((width, hid), F32),
            jax.ShapeDtypeStruct((hid, width), F32),
        ),
        in_specs=[vm] * 8,
        out_specs=(vm, vm, vm, vm),
        scratch_shapes=[
            pltpu.VMEM((tokens, width), BF),
            pltpu.VMEM((slots, tokens), BF),
            pltpu.VMEM((slots, 1), F32),
            pltpu.VMEM((3, 2, plane * CAP, width), BF),
            pltpu.VMEM((5, 2, plane * CAP, part), BF),
            pltpu.VMEM((2, slots, width), BF),
            pltpu.VMEM((slots, width), BF),
            pltpu.VMEM((3, slots, part), BF),
            pltpu.VMEM((slots, part), BF),
            pltpu.VMEM((slots, part), BF),
            pltpu.VMEM((slots, hid), BF),
            pltpu.VMEM((slots, hid), BF),
            pltpu.VMEM((slots, hid), BF),
        ]
        + [dma8] * 12
        + [
            pltpu.SemaphoreType.DMA,
            pltpu.SemaphoreType.DMA,
            pltpu.SemaphoreType.DMA,
            pltpu.SemaphoreType.DMA((3,)),
        ],
        compiler_params=pltpu.CompilerParams(
            collective_id=0, has_side_effects=True, vmem_limit_bytes=62 * 1024 * 1024
        ),
    )(choice, scale, cot, stream, gain, wg, wu, wd)


def shards(
    cotangent,
    stream_in,
    norm_gain,
    out_gate,
    in_gate,
    conv_input,
    conv_taps,
    out_weight,
    expert_gate,
    expert_up,
    expert_down,
    expert_choice,
    route_scale,
):
    sp_size = lax.axis_size("sp")
    tp_size = lax.axis_size("tp")
    model_width = stream_in.shape[1]
    column_width = model_width // tp_size
    column_start = lax.axis_index("tp") * column_width
    token_grad, grad_gate, grad_up, grad_down = through_experts(
        expert_choice.T, route_scale.T, cotangent, stream_in, norm_gain[None], expert_gate[0], expert_up[0], expert_down[0], sp_size
    )
    stream = stream_in.astype(F32)
    inverse_rms = lax.rsqrt(jnp.mean(stream * stream, axis=-1, keepdims=True) + norm_eps)
    unit_stream = stream * inverse_rms
    product = in_gate.astype(F32) * conv_input.astype(F32)
    earlier = passed_along(product[-2:], "sp", 1)
    extended = jnp.concatenate([earlier, product], axis=0)
    filtered = conv_taps[0] * product + conv_taps[1] * extended[1:-1] + conv_taps[2] * extended[:-2]
    mixed_in = (out_gate.astype(F32) * filtered).astype(BF)
    unit_grad = token_grad.astype(F32) * norm_gain
    along = jnp.mean(unit_stream * unit_grad, axis=-1, keepdims=True)
    stream_grad = (cotangent.astype(F32) + inverse_rms * (unit_grad - unit_stream * along)).astype(BF)
    grad_stream = lax.dynamic_slice_in_dim(stream_grad, column_start, column_width, 1)
    mixed_grad = jnp.dot(stream_grad, out_weight, preferred_element_type=F32)
    grad_out_gate = (mixed_grad * filtered).astype(BF)
    filtered_grad = mixed_grad * out_gate.astype(F32)
    later = passed_along(filtered_grad[:2], "sp", -1)
    extended_grad = jnp.concatenate([filtered_grad, later], axis=0)
    product_grad = (
        conv_taps[0] * filtered_grad
        + conv_taps[1] * extended_grad[1:-1]
        + conv_taps[2] * extended_grad[2:]
    )
    grad_in_gate = (product_grad * conv_input.astype(F32)).astype(BF)
    grad_conv_input = (product_grad * in_gate.astype(F32)).astype(BF)
    grad_out_weight = sent_and_summed(rows_product(stream_grad, mixed_in).astype(BF), "sp", 0)
    return (
        grad_stream,
        grad_out_gate,
        grad_in_gate,
        grad_conv_input,
        grad_out_weight,
        grad_gate[None],
        grad_up[None],
        grad_down[None],
    )


def solution(mesh):
    placed = (
        P("sp", None),
        P("sp", None),
        P(),
        P("sp", "tp"),
        P("sp", "tp"),
        P("sp", "tp"),
        P(None, "tp"),
        P(None, "tp"),
        P("sp", None, "tp"),
        P("sp", None, "tp"),
        P("sp", "tp", None),
        P("sp", None),
        P("sp", None),
    )
    return jax.shard_map(
        shards,
        mesh=mesh,
        in_specs=placed,
        out_specs=(
            P("sp", "tp"),
            P("sp", "tp"),
            P("sp", "tp"),
            P("sp", "tp"),
            P("sp", "tp"),
            P("sp", None, "tp"),
            P("sp", None, "tp"),
            P("sp", "tp", None),
        ),
        check_vma=False,
    )
```

```python
import functools

import jax
import jax.numpy as jnp
from jax import lax
from jax.experimental import pallas as pl
from jax.experimental.pallas import tpu as pltpu
from jax.sharding import PartitionSpec as P

norm_eps = 1e-06
MESH = pl.DeviceIdType.MESH
CAP = 16
BF = jnp.bfloat16
F32 = jnp.float32


def rows_product(left, right):
    return lax.dot_general(left, right, (((0,), (0,)), ((), ())), preferred_element_type=F32)


def cols_product(left, right):
    return lax.dot_general(left, right, (((1,), (1,)), ((), ())), preferred_element_type=F32)


def product_of(left, right):
    return jnp.dot(left, right, preferred_element_type=F32)


def loop(low, high, body):
    def step(i, carry):
        body(i)
        return carry

    lax.fori_loop(low, high, step, 0)


def offset_of(t):
    half = lax.div(t + 1, 2)
    odd = lax.rem(t, 2)
    spread = odd * (1 + half) + (1 - odd) * (7 - half)
    return spread + 7 * lax.div(t + 7, 8) - 7 + 3 * lax.div(t, 6) - 7 * lax.div(t, 7)


def rows_at(index, count):
    return pl.ds(pl.multiple_of(index * count, count), count)


def step_kernel(
    plane, choice, scale, cot, stream, gain, og, ig, ci, taps, wg_hbm, wu_hbm, wd_hbm, ow_hbm,
    out_stream, out_og, out_ig, out_ci, out_ow, out_gate, out_up, out_down,
    wg, wu, wd, ow, inverse, normed, pick, weight, send_all, send_part, rows, partial, summand, total, back,
    hidden, ggrad, ugrad, gate_out, up_out, down_out, tok, sgrad, extended, filtered, mixed, fgrad,
    owp, pair, psum, arrived,
    in_sem, out_sem,
    a_send, a_recv, right_send, left_send, from_left, from_right,
    fright_send, fleft_send, ffrom_left, ffrom_right,
    rs_send, rs_recv, tright_send, tleft_send, tfrom_left, tfrom_right, tf_send, tf_recv, one_send, one_recv,
):
    me = lax.axis_index("sp")
    q = lax.axis_index("tp")
    right = lax.rem(q + 1, 4)
    left = lax.rem(q + 3, 4)
    z = lax.div(me, plane)
    place = lax.rem(me, plane)
    experts = 8 * plane
    span = plane * CAP
    tokens, width = cot.shape
    part = width // 4
    mine = rows_at(q, part)
    of_left = rows_at(left, part)
    of_right = rows_at(right, part)
    of_far = rows_at(lax.rem(q + 2, 4), part)
    my_slots = rows_at(me, CAP)

    def copy_to(src, dst, send, recv, sp, tp):
        pltpu.make_async_remote_copy(src, dst, send, recv, device_id=(sp, tp), device_id_type=MESH).start()

    def wait_for(ref, sem):
        pltpu.make_async_copy(ref, ref, sem).wait()

    def source_at(t):
        return lax.rem(z + 8 - offset_of(t), 8)

    def next_place(k):
        return lax.rem(place + k, plane)

    weights = (
        pltpu.make_async_copy(wg_hbm, wg, in_sem.at[0]),
        pltpu.make_async_copy(wu_hbm, wu, in_sem.at[1]),
        pltpu.make_async_copy(wd_hbm, wd, in_sem.at[2]),
        pltpu.make_async_copy(ow_hbm, ow, in_sem.at[3]),
    )
    for copy in weights:
        copy.start()

    barrier = pltpu.get_barrier_semaphore()

    def greet(k):
        pl.semaphore_signal(barrier, inc=1, device_id=(lax.rem(me + k, experts), q), device_id_type=MESH)

    loop(1, experts, greet)

    def greet_row(k):
        pl.semaphore_signal(barrier, inc=1, device_id=(me, lax.rem(q + k, 4)), device_id_type=MESH)

    loop(1, 4, greet_row)

    def norm_rows(r):
        at = rows_at(r, 16)
        x = stream[at, :].astype(F32)
        inv = lax.rsqrt(jnp.mean(x * x, axis=-1, keepdims=True) + norm_eps)
        inverse[at, :] = inv
        normed[at, :] = ((x * inv) * gain[...]).astype(BF)

    loop(0, tokens // 16, norm_rows)

    first, second = choice[0:1, :], choice[1:2, :]
    ids = lax.broadcasted_iota(jnp.int32, (experts, tokens), 0)
    is_first, is_second = ids == first, ids == second
    named = jnp.where(is_first | is_second, 1.0, 0.0).astype(BF)
    before = jnp.where(
        lax.broadcasted_iota(jnp.int32, (tokens, tokens), 0) < lax.broadcasted_iota(jnp.int32, (tokens, tokens), 1), 1.0, 0.0
    ).astype(BF)
    earlier = product_of(named, before)
    slot_first = first * CAP + jnp.sum(jnp.where(is_first, earlier, 0.0), axis=0, keepdims=True).astype(jnp.int32)
    slot_second = second * CAP + jnp.sum(jnp.where(is_second, earlier, 0.0), axis=0, keepdims=True).astype(jnp.int32)

    def pick_rows(p):
        slots = lax.broadcasted_iota(jnp.int32, (span, tokens), 0) + p * span
        at_first, at_second = slots == slot_first, slots == slot_second
        pick[rows_at(p, span), :] = jnp.where(at_first | at_second, 1.0, 0.0).astype(BF)
        weight[rows_at(p, span), :] = jnp.sum(
            jnp.where(at_first, scale[0:1, :], 0.0) + jnp.where(at_second, scale[1:2, :], 0.0), axis=1, keepdims=True
        )

    loop(0, 8, pick_rows)

    def fill_quarter(t):
        at = rows_at(lax.rem(z + offset_of(t), 8), span)
        chosen = pick[at, :]
        send_part[t - 1, 0] = product_of(chosen, normed[:, mine]).astype(BF)
        send_part[t - 1, 1] = (product_of(chosen, cot[:, mine]) * weight[at, :]).astype(BF)

    loop(1, 6, fill_quarter)

    def turn_of(i):
        return i + 5 * lax.div(i + 1, 2)

    def fill_whole(i):
        at = rows_at(lax.rem(z + offset_of(turn_of(i)), 8), span)
        chosen = pick[at, :]
        send_all[i, 0] = product_of(chosen, normed[...]).astype(BF)
        send_all[i, 1] = (product_of(chosen, cot[...]) * weight[at, :]).astype(BF)

    loop(0, 3, fill_whole)
    own = rows_at(place, CAP)
    rows[0, my_slots, :] = send_all[0, 0, own, :]
    rows[1, my_slots, :] = send_all[0, 1, own, :]

    extended[8 : tokens + 8, :] = ig[...].astype(F32) * ci[...].astype(F32)

    @pl.when(me == 0)
    def _():
        extended[0:8, :] = jnp.zeros((8, part_of(extended)), F32)

    pl.semaphore_wait(barrier, experts + 2)

    @pl.when(me < experts - 1)
    def _():
        copy_to(extended.at[tokens : tokens + 8], extended.at[0:8], one_send.at[0], one_recv.at[0], me + 1, q)

    def send_quarter(t):
        target = lax.rem(z + offset_of(t), 8)

        def one(k):
            to = next_place(k)
            copy_to(
                send_part.at[t - 1, :, rows_at(to, CAP), :], rows.at[:, my_slots, mine],
                a_send.at[t], a_recv.at[t], target * plane + to, q,
            )

        loop(0, plane, one)

    loop(1, 6, send_quarter)

    def send_whole(i):
        t = turn_of(i)
        target = lax.rem(z + offset_of(t), 8)

        def one(k):
            to = next_place(k)

            @pl.when(target * plane + to != me)
            def _():
                copy_to(
                    send_all.at[i, :, rows_at(to, CAP), :], rows.at[:, my_slots, :],
                    a_send.at[t], a_recv.at[t], target * plane + to, q,
                )

        loop(0, plane, one)

    loop(0, 3, send_whole)

    @pl.when(me > 0)
    def _():
        wait_for(extended.at[0:8], one_recv.at[0])

    now = (
        taps[0:1, :] * extended[8 : tokens + 8, :]
        + taps[1:2, :] * extended[7 : tokens + 7, :]
        + taps[2:3, :] * extended[6 : tokens + 6, :]
    )
    filtered[...] = now
    mixed[...] = (og[...].astype(F32) * now).astype(BF)
    for copy in weights:
        copy.wait()

    def step(i):
        @pl.when((i >= 1) & (i < 6))
        def _():
            piece = rows.at[:, rows_at(source_at(i), span), mine]
            wait_for(piece, a_recv.at[i])
            copy_to(piece, piece, right_send.at[i], from_left.at[i], me, right)
            copy_to(piece, piece, left_send.at[i], from_right.at[i], me, left)

        @pl.when((i >= 2) & (i < 7))
        def _():
            t = i - 1
            at = rows_at(source_at(t), span)
            wait_for(rows.at[:, at, of_left], from_left.at[t])
            half = rows.at[0, at, of_left]
            copy_to(half, half, fright_send.at[t], ffrom_left.at[t], me, right)
            wait_for(rows.at[:, at, of_right], from_right.at[t])
            half = rows.at[1, at, of_right]
            copy_to(half, half, fleft_send.at[t], ffrom_right.at[t], me, left)

        @pl.when((i == 0) | ((i >= 3) & (i < 10)))
        def _():
            t = (i - 2) * lax.div(i + 13, 16)
            at = rows_at(source_at(t), span)

            @pl.when((t >= 1) & (t < 6))
            def _():
                wait_for(rows.at[0, at, of_far], ffrom_left.at[t])
                wait_for(rows.at[1, at, of_far], ffrom_right.at[t])

            @pl.when(t == 0)
            def _():
                if plane > 1:
                    wait_for(rows.at[:, pl.ds(0, (plane - 1) * CAP), :], a_recv.at[0])

            @pl.when(t >= 6)
            def _():
                wait_for(rows.at[:, at, :], a_recv.at[t])

            here = rows[0, at, :]
            gate_pre = product_of(here, wg[...])
            up_pre = product_of(here, wu[...])
            hidden_grad = cols_product(rows[1, at, :], wd[...])
            sigmoid_gate = jax.nn.sigmoid(gate_pre)
            silu_gate = gate_pre * sigmoid_gate
            hidden[at, :] = (silu_gate * up_pre).astype(BF)
            gate_grad = (hidden_grad * up_pre * sigmoid_gate * (1.0 + gate_pre * (1.0 - sigmoid_gate))).astype(BF)
            up_grad = (hidden_grad * silu_gate).astype(BF)
            ggrad[at, :] = gate_grad
            ugrad[at, :] = up_grad
            partial[at, :] = (cols_product(gate_grad, wg[...]) + cols_product(up_grad, wu[...])).astype(BF)

            def one(d):
                to = lax.rem(q + d, 4)
                copy_to(partial.at[at, rows_at(to, part)], summand.at[d - 1, at, :], rs_send.at[t], rs_recv.at[t], me, to)

            loop(1, 4, one)

        @pl.when(i >= 3)
        def _():
            t = i - 3
            source = source_at(t)
            at = rows_at(source, span)
            wait_for(summand.at[:, at, :], rs_recv.at[t])
            added = partial[at, mine].astype(F32)
            for d in range(3):
                added = added + summand[d, at, :].astype(F32)
            total[at, :] = added.astype(BF)

            def one(k):
                to = source * plane + next_place(k)

                @pl.when(to != me)
                def _():
                    copy_to(total.at[rows_at(to, CAP), :], back.at[my_slots, :], one_send.at[1], one_recv.at[1], to, q)

            loop(0, plane, one)

    loop(0, 11, step)
    back[my_slots, :] = total[my_slots, :]

    chunk = min(256, width)

    def grads(m):
        cols = rows_at(m, chunk)
        here = rows[0, :, cols]
        gate_out[cols, :] = rows_product(here, ggrad[...]).astype(BF)
        up_out[cols, :] = rows_product(here, ugrad[...]).astype(BF)
        down_out[:, cols] = rows_product(hidden[...], rows[1, :, cols]).astype(BF)

    loop(0, width // chunk, grads)
    finished = (
        pltpu.make_async_copy(gate_out, out_gate, out_sem.at[0]),
        pltpu.make_async_copy(up_out, out_up, out_sem.at[1]),
        pltpu.make_async_copy(down_out, out_down, out_sem.at[2]),
    )
    for copy in finished:
        copy.start()

    wait_for(back.at[pl.ds(0, (experts - 1) * CAP), :], one_recv.at[1])
    tok[:, mine] = rows_product(pick[...], back[...]).astype(BF)
    half = tokens // 2
    low, high = pl.ds(0, half), pl.ds(half, half)
    for h, at in ((0, low), (1, high)):
        copy_to(tok.at[at, mine], tok.at[at, mine], tright_send.at[h], tfrom_left.at[h], me, right)
    for h, at in ((1, high), (0, low)):
        copy_to(tok.at[at, mine], tok.at[at, mine], tleft_send.at[h], tfrom_right.at[h], me, left)
    wait_for(tok.at[low, of_left], tfrom_left.at[0])
    copy_to(tok.at[low, of_left], tok.at[low, of_left], tf_send.at[0], tf_recv.at[0], me, right)
    wait_for(tok.at[high, of_right], tfrom_right.at[1])
    copy_to(tok.at[high, of_right], tok.at[high, of_right], tf_send.at[1], tf_recv.at[1], me, left)
    wait_for(tok.at[high, of_left], tfrom_left.at[1])
    wait_for(tok.at[low, of_right], tfrom_right.at[0])
    wait_for(tok.at[low, of_far], tf_recv.at[0])
    wait_for(tok.at[high, of_far], tf_recv.at[1])

    def stream_rows(r):
        at = rows_at(r, 16)
        inv = inverse[at, :]
        unit = stream[at, :].astype(F32) * inv
        unit_grad = tok[at, :].astype(F32) * gain[...]
        along = jnp.mean(unit * unit_grad, axis=-1, keepdims=True)
        sgrad[at, :] = (cot[at, :].astype(F32) + inv * (unit_grad - unit * along)).astype(BF)

    loop(0, tokens // 16, stream_rows)

    block = width // experts
    pairs = experts // 2
    core = lax.rem(me, 2)
    here = lax.div(me, 2)
    chunks = min(8, pairs)
    groups = pairs // chunks
    cut = 2 * groups * block

    def out_rows(m):
        found = rows_product(sgrad[:, rows_at(m, cut)], mixed[...]).astype(BF)
        owp[rows_at(m, groups)] = found.reshape(groups, 2, block, found.shape[-1])

    loop(0, chunks, out_rows)
    copy_to(owp.at[:, 1 - core], pair, one_send.at[2], one_recv.at[2], me + 1 - 2 * core, q)

    mixed_grad = product_of(sgrad[...], ow[...])
    out_og[...] = (mixed_grad * filtered[...]).astype(BF)
    fgrad[0:tokens, :] = mixed_grad * og[...].astype(F32)

    @pl.when(me > 0)
    def _():
        copy_to(fgrad.at[0:8], fgrad.at[tokens : tokens + 8], one_send.at[3], one_recv.at[3], me - 1, q)

    @pl.when(me == experts - 1)
    def _():
        fgrad[tokens : tokens + 8, :] = jnp.zeros((8, part_of(fgrad)), F32)

    wait_for(pair, one_recv.at[2])

    def pair_sum(m):
        at = rows_at(m, groups)
        psum[at] = (owp[at, core].astype(F32) + pair[at].astype(F32)).astype(BF)

    loop(0, chunks, pair_sum)

    def send_sum(k):
        to = lax.rem(here + k, pairs)
        copy_to(psum.at[to], arrived.at[here], one_send.at[4], one_recv.at[4], 2 * to + core, q)

    loop(1, pairs, send_sum)
    arrived[here] = psum[here]
    out_stream[...] = sgrad[:, mine]

    @pl.when(me < experts - 1)
    def _():
        wait_for(fgrad.at[tokens : tokens + 8], one_recv.at[3])

    product_grad = (
        taps[0:1, :] * fgrad[0:tokens, :] + taps[1:2, :] * fgrad[1 : tokens + 1, :] + taps[2:3, :] * fgrad[2 : tokens + 2, :]
    )
    out_ig[...] = (product_grad * ci[...].astype(F32)).astype(BF)
    out_ci[...] = (product_grad * ig[...].astype(F32)).astype(BF)

    def sent_rows(t):
        @pl.when((t >= 1) & (t < 6))
        def _():
            piece = rows.at[:, rows_at(0, span), mine]
            wait_for(piece, a_send.at[t])
            wait_for(piece, right_send.at[t])
            wait_for(piece, left_send.at[t])
            wait_for(rows.at[0, rows_at(0, span), mine], fright_send.at[t])
            wait_for(rows.at[0, rows_at(0, span), mine], fleft_send.at[t])

        @pl.when(t == 0)
        def _():
            if plane > 1:
                wait_for(rows.at[:, pl.ds(0, (plane - 1) * CAP), :], a_send.at[0])

        @pl.when(t >= 6)
        def _():
            wait_for(rows.at[:, rows_at(0, span), :], a_send.at[t])

        wait_for(summand.at[:, rows_at(0, span), :], rs_send.at[t])

    loop(0, 8, sent_rows)
    wait_for(back.at[pl.ds(0, (experts - 1) * CAP), :], one_send.at[1])
    for h in range(2):
        wait_for(tok.at[low, mine], tright_send.at[h])
        wait_for(tok.at[low, mine], tleft_send.at[h])
        wait_for(tok.at[low, mine], tf_send.at[h])
    wait_for(pair, one_send.at[2])

    @pl.when(me < experts - 1)
    def _():
        wait_for(extended.at[0:8], one_send.at[0])

    @pl.when(me > 0)
    def _():
        wait_for(fgrad.at[0:8], one_send.at[3])

    for copy in finished:
        copy.wait()
    wait_for(arrived.at[pl.ds(0, pairs - 1)], one_recv.at[4])
    added = arrived[0].astype(F32)
    for p in range(1, pairs):
        added = added + arrived[p].astype(F32)
    out_ow[...] = added
    wait_for(arrived.at[pl.ds(0, pairs - 1)], one_send.at[4])


def part_of(ref):
    return ref.shape[-1]


def whole_step(choice, scale, cot, stream, gain, og, ig, ci, taps, wg, wu, wd, ow, experts):
    tokens, width = cot.shape
    part = width // 4
    slots = experts * CAP
    plane = experts // 8
    hid = wg.shape[1]
    chan = og.shape[1]
    block = width // experts
    vm = pl.BlockSpec(memory_space=pltpu.VMEM)
    hbm = pl.BlockSpec(memory_space=pltpu.HBM)
    dma = pltpu.SemaphoreType.DMA
    return pl.pallas_call(
        functools.partial(step_kernel, plane),
        name="experts",
        out_shape=(
            jax.ShapeDtypeStruct((tokens, part), BF),
            jax.ShapeDtypeStruct((tokens, chan), BF),
            jax.ShapeDtypeStruct((tokens, chan), BF),
            jax.ShapeDtypeStruct((tokens, chan), BF),
            jax.ShapeDtypeStruct((block, chan), F32),
            jax.ShapeDtypeStruct((width, hid), BF),
            jax.ShapeDtypeStruct((width, hid), BF),
            jax.ShapeDtypeStruct((hid, width), BF),
        ),
        in_specs=[vm] * 9 + [hbm] * 4,
        out_specs=(vm,) * 5 + (hbm,) * 3,
        scratch_shapes=[
            pltpu.VMEM((width, hid), BF),
            pltpu.VMEM((width, hid), BF),
            pltpu.VMEM((hid, width), BF),
            pltpu.VMEM((width, chan), BF),
            pltpu.VMEM((tokens, 1), F32),
            pltpu.VMEM((tokens, width), BF),
            pltpu.VMEM((slots, tokens), BF),
            pltpu.VMEM((slots, 1), F32),
            pltpu.VMEM((3, 2, plane * CAP, width), BF),
            pltpu.VMEM((5, 2, plane * CAP, part), BF),
            pltpu.VMEM((2, slots, width), BF),
            pltpu.VMEM((slots, width), BF),
            pltpu.VMEM((3, slots, part), BF),
            pltpu.VMEM((slots, part), BF),
            pltpu.VMEM((slots, part), BF),
            pltpu.VMEM((slots, hid), BF),
            pltpu.VMEM((slots, hid), BF),
            pltpu.VMEM((slots, hid), BF),
            pltpu.VMEM((width, hid), BF),
            pltpu.VMEM((width, hid), BF),
            pltpu.VMEM((hid, width), BF),
            pltpu.VMEM((tokens, width), BF),
            pltpu.VMEM((tokens, width), BF),
            pltpu.VMEM((tokens + 8, chan), F32),
            pltpu.VMEM((tokens, chan), F32),
            pltpu.VMEM((tokens, chan), BF),
            pltpu.VMEM((tokens + 8, chan), F32),
            pltpu.VMEM((experts // 2, 2, block, chan), BF),
            pltpu.VMEM((experts // 2, block, chan), BF),
            pltpu.VMEM((experts // 2, block, chan), BF),
            pltpu.VMEM((experts // 2, block, chan), BF),
            dma((4,)),
            dma((3,)),
        ]
        + [dma((8,))] * 12
        + [dma((2,))] * 6
        + [dma((5,))] * 2,
        compiler_params=pltpu.CompilerParams(
            collective_id=0, has_side_effects=True, vmem_limit_bytes=62 * 1024 * 1024
        ),
    )(choice, scale, cot, stream, gain, og, ig, ci, taps, wg, wu, wd, ow)


def shards(
    cotangent,
    stream_in,
    norm_gain,
    out_gate,
    in_gate,
    conv_input,
    conv_taps,
    out_weight,
    expert_gate,
    expert_up,
    expert_down,
    expert_choice,
    route_scale,
):
    sp_size = lax.axis_size("sp")
    *others, grad_gate, grad_up, grad_down = whole_step(
        expert_choice.T, route_scale.T, cotangent, stream_in, norm_gain[None], out_gate, in_gate, conv_input, conv_taps,
        expert_gate[0], expert_up[0], expert_down[0], out_weight, sp_size,
    )
    return (*others, grad_gate[None].astype(F32), grad_up[None].astype(F32), grad_down[None].astype(F32))


def solution(mesh):
    placed = (
        P("sp", None),
        P("sp", None),
        P(),
        P("sp", "tp"),
        P("sp", "tp"),
        P("sp", "tp"),
        P(None, "tp"),
        P(None, "tp"),
        P("sp", None, "tp"),
        P("sp", None, "tp"),
        P("sp", "tp", None),
        P("sp", None),
        P("sp", None),
    )
    return jax.shard_map(
        shards,
        mesh=mesh,
        in_specs=placed,
        out_specs=(
            P("sp", "tp"),
            P("sp", "tp"),
            P("sp", "tp"),
            P("sp", "tp"),
            P("sp", "tp"),
            P("sp", None, "tp"),
            P("sp", None, "tp"),
            P("sp", "tp", None),
        ),
        check_vma=False,
    )
```

```python
import functools

import jax
import jax.numpy as jnp
from jax import lax
from jax.experimental import pallas as pl
from jax.experimental.pallas import tpu as pltpu
from jax.sharding import PartitionSpec as P

norm_eps = 1e-06
MESH = pl.DeviceIdType.MESH
CAP = 16
BF = jnp.bfloat16
F32 = jnp.float32


def rows_product(left, right):
    return lax.dot_general(left, right, (((0,), (0,)), ((), ())), preferred_element_type=F32)


def cols_product(left, right):
    return lax.dot_general(left, right, (((1,), (1,)), ((), ())), preferred_element_type=F32)


def product_of(left, right):
    return jnp.dot(left, right, preferred_element_type=F32)


def loop(low, high, body):
    def step(i, carry):
        body(i)
        return carry

    lax.fori_loop(low, high, step, 0)


def offset_of(t):
    half = lax.div(t + 1, 2)
    odd = lax.rem(t, 2)
    spread = odd * (1 + half) + (1 - odd) * (7 - half)
    return spread + 7 * lax.div(t + 7, 8) - 7 + 3 * lax.div(t, 6) - 7 * lax.div(t, 7)


def rows_at(index, count):
    return pl.ds(pl.multiple_of(index * count, count), count)


def step_kernel(
    plane, choice, scale, cot, stream, gain, og, ig, ci, taps, wg_hbm, wu_hbm, wd_hbm, ow_hbm,
    out_stream, out_og, out_ig, out_ci, out_ow, out_gate, out_up, out_down,
    wg, wu, wd, ow, inverse, normed, pick, weight, send_all, send_part, rows, partial, summand, total, back,
    hidden, ggrad, ugrad, gate_out, up_out, down_out, tok, sgrad, extended, filtered, mixed, fgrad,
    owp, pair, psum, arrived, gate_sum, up_sum, down_sum,
    in_sem, out_sem,
    a_send, a_recv, right_send, left_send, from_left, from_right,
    fright_send, fleft_send, ffrom_left, ffrom_right,
    rs_send, rs_recv, tright_send, tleft_send, tfrom_left, tfrom_right, tf_send, tf_recv, one_send, one_recv, pair_send, pair_recv,
):
    me = lax.axis_index("sp")
    q = lax.axis_index("tp")
    right = lax.rem(q + 1, 4)
    left = lax.rem(q + 3, 4)
    z = lax.div(me, plane)
    place = lax.rem(me, plane)
    experts = 8 * plane
    span = plane * CAP
    tokens, width = cot.shape
    part = width // 4
    mine = rows_at(q, part)
    of_left = rows_at(left, part)
    of_right = rows_at(right, part)
    of_far = rows_at(lax.rem(q + 2, 4), part)
    my_slots = rows_at(me, CAP)

    def copy_to(src, dst, send, recv, sp, tp):
        pltpu.make_async_remote_copy(src, dst, send, recv, device_id=(sp, tp), device_id_type=MESH).start()

    def wait_for(ref, sem):
        pltpu.make_async_copy(ref, ref, sem).wait()

    def source_at(t):
        return lax.rem(z + 8 - offset_of(t), 8)

    def next_place(k):
        return lax.rem(place + k, plane)

    weights = (
        pltpu.make_async_copy(wg_hbm, wg, in_sem.at[0]),
        pltpu.make_async_copy(wu_hbm, wu, in_sem.at[1]),
        pltpu.make_async_copy(wd_hbm, wd, in_sem.at[2]),
        pltpu.make_async_copy(ow_hbm, ow, in_sem.at[3]),
    )
    for copy in weights:
        copy.start()

    barrier = pltpu.get_barrier_semaphore()

    def greet(k):
        pl.semaphore_signal(barrier, inc=1, device_id=(lax.rem(me + k, experts), q), device_id_type=MESH)

    loop(1, experts, greet)

    def greet_row(k):
        pl.semaphore_signal(barrier, inc=1, device_id=(me, lax.rem(q + k, 4)), device_id_type=MESH)

    loop(1, 4, greet_row)

    def norm_rows(r):
        at = rows_at(r, 16)
        x = stream[at, :].astype(F32)
        inv = lax.rsqrt(jnp.mean(x * x, axis=-1, keepdims=True) + norm_eps)
        inverse[at, :] = inv
        normed[at, :] = ((x * inv) * gain[...]).astype(BF)

    loop(0, tokens // 16, norm_rows)

    first, second = choice[0:1, :], choice[1:2, :]
    ids = lax.broadcasted_iota(jnp.int32, (experts, tokens), 0)
    is_first, is_second = ids == first, ids == second
    named = jnp.where(is_first | is_second, 1.0, 0.0).astype(BF)
    before = jnp.where(
        lax.broadcasted_iota(jnp.int32, (tokens, tokens), 0) < lax.broadcasted_iota(jnp.int32, (tokens, tokens), 1), 1.0, 0.0
    ).astype(BF)
    earlier = product_of(named, before)
    slot_first = first * CAP + jnp.sum(jnp.where(is_first, earlier, 0.0), axis=0, keepdims=True).astype(jnp.int32)
    slot_second = second * CAP + jnp.sum(jnp.where(is_second, earlier, 0.0), axis=0, keepdims=True).astype(jnp.int32)

    def pick_rows(p):
        slots = lax.broadcasted_iota(jnp.int32, (span, tokens), 0) + p * span
        at_first, at_second = slots == slot_first, slots == slot_second
        pick[rows_at(p, span), :] = jnp.where(at_first | at_second, 1.0, 0.0).astype(BF)
        weight[rows_at(p, span), :] = jnp.sum(
            jnp.where(at_first, scale[0:1, :], 0.0) + jnp.where(at_second, scale[1:2, :], 0.0), axis=1, keepdims=True
        )

    loop(0, 8, pick_rows)

    def fill_quarter(t):
        at = rows_at(lax.rem(z + offset_of(t), 8), span)
        chosen = pick[at, :]
        send_part[t - 1, 0] = product_of(chosen, normed[:, mine]).astype(BF)
        send_part[t - 1, 1] = (product_of(chosen, cot[:, mine]) * weight[at, :]).astype(BF)

    loop(1, 6, fill_quarter)

    extended[8 : tokens + 8, :] = ig[...].astype(F32) * ci[...].astype(F32)

    @pl.when(me == 0)
    def _():
        extended[0:8, :] = jnp.zeros((8, part_of(extended)), F32)

    pl.semaphore_wait(barrier, experts + 2)

    @pl.when(me < experts - 1)
    def _():
        copy_to(extended.at[tokens : tokens + 8], extended.at[0:8], one_send.at[0], one_recv.at[0], me + 1, q)

    def send_quarter(t):
        target = lax.rem(z + offset_of(t), 8)

        def one(k):
            to = next_place(k)
            copy_to(
                send_part.at[t - 1, :, rows_at(to, CAP), :], rows.at[:, my_slots, mine],
                a_send.at[t], a_recv.at[t], target * plane + to, q,
            )

        loop(0, plane, one)

    loop(1, 6, send_quarter)

    def turn_of(i):
        return i + 5 * lax.div(i + 1, 2)

    def fill_whole(i):
        at = rows_at(lax.rem(z + offset_of(turn_of(i)), 8), span)
        chosen = pick[at, :]
        send_all[i, 0] = product_of(chosen, normed[...]).astype(BF)
        send_all[i, 1] = (product_of(chosen, cot[...]) * weight[at, :]).astype(BF)

    loop(0, 3, fill_whole)
    own = rows_at(place, CAP)
    rows[0, my_slots, :] = send_all[0, 0, own, :]
    rows[1, my_slots, :] = send_all[0, 1, own, :]

    def send_whole(i):
        t = turn_of(i)
        target = lax.rem(z + offset_of(t), 8)

        def one(k):
            to = next_place(k)

            @pl.when(target * plane + to != me)
            def _():
                copy_to(
                    send_all.at[i, :, rows_at(to, CAP), :], rows.at[:, my_slots, :],
                    a_send.at[t], a_recv.at[t], target * plane + to, q,
                )

        loop(0, plane, one)

    loop(0, 3, send_whole)

    @pl.when(me > 0)
    def _():
        wait_for(extended.at[0:8], one_recv.at[0])

    now = (
        taps[0:1, :] * extended[8 : tokens + 8, :]
        + taps[1:2, :] * extended[7 : tokens + 7, :]
        + taps[2:3, :] * extended[6 : tokens + 6, :]
    )
    filtered[...] = now
    mixed[...] = (og[...].astype(F32) * now).astype(BF)
    chunk = min(256, width)

    def clear(m):
        cols = rows_at(m, chunk)
        gate_sum[cols, :] = jnp.zeros((chunk, part_of(gate_sum)), F32)
        up_sum[cols, :] = jnp.zeros((chunk, part_of(up_sum)), F32)
        down_sum[:, cols] = jnp.zeros((down_sum.shape[0], chunk), F32)

    loop(0, width // chunk, clear)
    for copy in weights:
        copy.wait()

    def step(i):
        @pl.when((i >= 1) & (i < 6))
        def _():
            piece = rows.at[:, rows_at(source_at(i), span), mine]
            wait_for(piece, a_recv.at[i])
            copy_to(piece, piece, right_send.at[i], from_left.at[i], me, right)
            copy_to(piece, piece, left_send.at[i], from_right.at[i], me, left)

        @pl.when((i >= 2) & (i < 7))
        def _():
            t = i - 1
            at = rows_at(source_at(t), span)
            wait_for(rows.at[:, at, of_left], from_left.at[t])
            half = rows.at[0, at, of_left]
            copy_to(half, half, fright_send.at[t], ffrom_left.at[t], me, right)
            wait_for(rows.at[:, at, of_right], from_right.at[t])
            half = rows.at[1, at, of_right]
            copy_to(half, half, fleft_send.at[t], ffrom_right.at[t], me, left)

        @pl.when((i >= 2) & (i < 10))
        def _():
            t = i - 2
            at = rows_at(source_at(t), span)

            @pl.when((t >= 1) & (t < 6))
            def _():
                wait_for(rows.at[0, at, of_far], ffrom_left.at[t])
                wait_for(rows.at[1, at, of_far], ffrom_right.at[t])

            @pl.when(t == 0)
            def _():
                if plane > 1:
                    wait_for(rows.at[:, pl.ds(0, (plane - 1) * CAP), :], a_recv.at[0])

            @pl.when(t >= 6)
            def _():
                wait_for(rows.at[:, at, :], a_recv.at[t])

            here = rows[0, at, :]
            gate_pre = product_of(here, wg[...])
            up_pre = product_of(here, wu[...])
            hidden_grad = cols_product(rows[1, at, :], wd[...])
            sigmoid_gate = jax.nn.sigmoid(gate_pre)
            silu_gate = gate_pre * sigmoid_gate
            hidden[at, :] = (silu_gate * up_pre).astype(BF)
            gate_grad = (hidden_grad * up_pre * sigmoid_gate * (1.0 + gate_pre * (1.0 - sigmoid_gate))).astype(BF)
            up_grad = (hidden_grad * silu_gate).astype(BF)
            ggrad[at, :] = gate_grad
            ugrad[at, :] = up_grad
            partial[at, :] = (cols_product(gate_grad, wg[...]) + cols_product(up_grad, wu[...])).astype(BF)

            def one(d):
                to = lax.rem(q + d, 4)
                copy_to(partial.at[at, rows_at(to, part)], summand.at[d - 1, at, :], rs_send.at[t], rs_recv.at[t], me, to)

            loop(1, 4, one)

            def add_grads(m):
                cols = rows_at(m, chunk)
                rows_here = rows[0, at, cols]
                gate_sum[cols, :] += rows_product(rows_here, ggrad[at, :])
                up_sum[cols, :] += rows_product(rows_here, ugrad[at, :])
                down_sum[:, cols] += rows_product(hidden[at, :], rows[1, at, cols])

            loop(0, width // chunk, add_grads)

        @pl.when(i >= 3)
        def _():
            t = i - 3
            source = source_at(t)
            at = rows_at(source, span)
            wait_for(summand.at[:, at, :], rs_recv.at[t])
            added = partial[at, mine].astype(F32)
            for d in range(3):
                added = added + summand[d, at, :].astype(F32)
            total[at, :] = added.astype(BF)

            def one(k):
                to = source * plane + next_place(k)

                @pl.when(to != me)
                def _():
                    copy_to(total.at[rows_at(to, CAP), :], back.at[my_slots, :], one_send.at[1], one_recv.at[1], to, q)

            loop(0, plane, one)

    loop(1, 11, step)
    back[my_slots, :] = total[my_slots, :]

    def narrow(m):
        cols = rows_at(m, chunk)
        gate_out[cols, :] = gate_sum[cols, :].astype(BF)
        up_out[cols, :] = up_sum[cols, :].astype(BF)
        down_out[:, cols] = down_sum[:, cols].astype(BF)

    loop(0, width // chunk, narrow)
    finished = (
        pltpu.make_async_copy(gate_out, out_gate, out_sem.at[0]),
        pltpu.make_async_copy(up_out, out_up, out_sem.at[1]),
        pltpu.make_async_copy(down_out, out_down, out_sem.at[2]),
    )
    for copy in finished:
        copy.start()

    wait_for(back.at[pl.ds(0, (experts - 1) * CAP), :], one_recv.at[1])
    tok[:, mine] = rows_product(pick[...], back[...]).astype(BF)
    half = tokens // 2
    low, high = pl.ds(0, half), pl.ds(half, half)
    for h, at in ((0, low), (1, high)):
        copy_to(tok.at[at, mine], tok.at[at, mine], tright_send.at[h], tfrom_left.at[h], me, right)
    for h, at in ((1, high), (0, low)):
        copy_to(tok.at[at, mine], tok.at[at, mine], tleft_send.at[h], tfrom_right.at[h], me, left)
    wait_for(tok.at[low, of_left], tfrom_left.at[0])
    copy_to(tok.at[low, of_left], tok.at[low, of_left], tf_send.at[0], tf_recv.at[0], me, right)
    wait_for(tok.at[high, of_right], tfrom_right.at[1])
    copy_to(tok.at[high, of_right], tok.at[high, of_right], tf_send.at[1], tf_recv.at[1], me, left)
    wait_for(tok.at[high, of_left], tfrom_left.at[1])
    wait_for(tok.at[low, of_right], tfrom_right.at[0])
    wait_for(tok.at[low, of_far], tf_recv.at[0])
    wait_for(tok.at[high, of_far], tf_recv.at[1])

    def stream_rows(r):
        at = rows_at(r, 16)
        inv = inverse[at, :]
        unit = stream[at, :].astype(F32) * inv
        unit_grad = tok[at, :].astype(F32) * gain[...]
        along = jnp.mean(unit * unit_grad, axis=-1, keepdims=True)
        sgrad[at, :] = (cot[at, :].astype(F32) + inv * (unit_grad - unit * along)).astype(BF)

    loop(0, tokens // 16, stream_rows)

    block = width // experts
    pairs = experts // 2
    core = lax.rem(me, 2)
    here = lax.div(me, 2)
    groups = plane // 2
    cut = plane * block

    def plane_of(j):
        half = lax.div(j + 1, 2)
        return lax.rem(z + 4 + half - 2 * half * lax.rem(j, 2), 8)

    def out_rows(j):
        at = plane_of(j)
        found = rows_product(sgrad[:, rows_at(at, cut)], mixed[...]).astype(BF)
        of_plane = rows_at(at, groups)
        owp[of_plane] = found.reshape(groups, 2, block, found.shape[-1])
        copy_to(owp.at[of_plane, 1 - core], pair.at[of_plane], pair_send.at[j], pair_recv.at[j], me + 1 - 2 * core, q)

    loop(0, 8, out_rows)

    def pair_sum(j):
        at = plane_of(j)
        of_plane = rows_at(at, groups)
        wait_for(pair.at[of_plane], pair_recv.at[j])
        psum[of_plane] = (owp[of_plane, core].astype(F32) + pair[of_plane].astype(F32)).astype(BF)

        def send_sum(k):
            to = at * groups + lax.rem(here + k, groups)

            @pl.when(to != here)
            def _():
                copy_to(psum.at[to], arrived.at[here], one_send.at[4], one_recv.at[4], 2 * to + core, q)

        loop(0, groups, send_sum)

    loop(0, 8, pair_sum)
    arrived[here] = psum[here]

    mixed_grad = product_of(sgrad[...], ow[...])
    fgrad[0:tokens, :] = mixed_grad * og[...].astype(F32)

    @pl.when(me > 0)
    def _():
        copy_to(fgrad.at[0:8], fgrad.at[tokens : tokens + 8], one_send.at[3], one_recv.at[3], me - 1, q)

    @pl.when(me == experts - 1)
    def _():
        fgrad[tokens : tokens + 8, :] = jnp.zeros((8, part_of(fgrad)), F32)

    out_og[...] = (mixed_grad * filtered[...]).astype(BF)
    out_stream[...] = sgrad[:, mine]

    @pl.when(me < experts - 1)
    def _():
        wait_for(fgrad.at[tokens : tokens + 8], one_recv.at[3])

    product_grad = (
        taps[0:1, :] * fgrad[0:tokens, :] + taps[1:2, :] * fgrad[1 : tokens + 1, :] + taps[2:3, :] * fgrad[2 : tokens + 2, :]
    )
    out_ig[...] = (product_grad * ci[...].astype(F32)).astype(BF)
    out_ci[...] = (product_grad * ig[...].astype(F32)).astype(BF)

    def sent_rows(t):
        @pl.when((t >= 1) & (t < 6))
        def _():
            piece = rows.at[:, rows_at(0, span), mine]
            wait_for(piece, a_send.at[t])
            wait_for(piece, right_send.at[t])
            wait_for(piece, left_send.at[t])
            wait_for(rows.at[0, rows_at(0, span), mine], fright_send.at[t])
            wait_for(rows.at[0, rows_at(0, span), mine], fleft_send.at[t])

        @pl.when(t == 0)
        def _():
            if plane > 1:
                wait_for(rows.at[:, pl.ds(0, (plane - 1) * CAP), :], a_send.at[0])

        @pl.when(t >= 6)
        def _():
            wait_for(rows.at[:, rows_at(0, span), :], a_send.at[t])

        wait_for(summand.at[:, rows_at(0, span), :], rs_send.at[t])

    loop(0, 8, sent_rows)
    wait_for(back.at[pl.ds(0, (experts - 1) * CAP), :], one_send.at[1])
    for h in range(2):
        wait_for(tok.at[low, mine], tright_send.at[h])
        wait_for(tok.at[low, mine], tleft_send.at[h])
        wait_for(tok.at[low, mine], tf_send.at[h])

    def pair_sent(j):
        wait_for(pair.at[pl.ds(0, groups)], pair_send.at[j])

    loop(0, 8, pair_sent)

    @pl.when(me < experts - 1)
    def _():
        wait_for(extended.at[0:8], one_send.at[0])

    @pl.when(me > 0)
    def _():
        wait_for(fgrad.at[0:8], one_send.at[3])

    for copy in finished:
        copy.wait()
    wait_for(arrived.at[pl.ds(0, pairs - 1)], one_recv.at[4])
    added = arrived[0].astype(F32)
    for p in range(1, pairs):
        added = added + arrived[p].astype(F32)
    out_ow[...] = added
    wait_for(arrived.at[pl.ds(0, pairs - 1)], one_send.at[4])


def part_of(ref):
    return ref.shape[-1]


def whole_step(choice, scale, cot, stream, gain, og, ig, ci, taps, wg, wu, wd, ow, experts):
    tokens, width = cot.shape
    part = width // 4
    slots = experts * CAP
    plane = experts // 8
    hid = wg.shape[1]
    chan = og.shape[1]
    block = width // experts
    vm = pl.BlockSpec(memory_space=pltpu.VMEM)
    hbm = pl.BlockSpec(memory_space=pltpu.HBM)
    dma = pltpu.SemaphoreType.DMA
    return pl.pallas_call(
        functools.partial(step_kernel, plane),
        name="experts",
        out_shape=(
            jax.ShapeDtypeStruct((tokens, part), BF),
            jax.ShapeDtypeStruct((tokens, chan), BF),
            jax.ShapeDtypeStruct((tokens, chan), BF),
            jax.ShapeDtypeStruct((tokens, chan), BF),
            jax.ShapeDtypeStruct((block, chan), F32),
            jax.ShapeDtypeStruct((width, hid), BF),
            jax.ShapeDtypeStruct((width, hid), BF),
            jax.ShapeDtypeStruct((hid, width), BF),
        ),
        in_specs=[vm] * 9 + [hbm] * 4,
        out_specs=(vm,) * 5 + (hbm,) * 3,
        scratch_shapes=[
            pltpu.VMEM((width, hid), BF),
            pltpu.VMEM((width, hid), BF),
            pltpu.VMEM((hid, width), BF),
            pltpu.VMEM((width, chan), BF),
            pltpu.VMEM((tokens, 1), F32),
            pltpu.VMEM((tokens, width), BF),
            pltpu.VMEM((slots, tokens), BF),
            pltpu.VMEM((slots, 1), F32),
            pltpu.VMEM((3, 2, plane * CAP, width), BF),
            pltpu.VMEM((5, 2, plane * CAP, part), BF),
            pltpu.VMEM((2, slots, width), BF),
            pltpu.VMEM((slots, width), BF),
            pltpu.VMEM((3, slots, part), BF),
            pltpu.VMEM((slots, part), BF),
            pltpu.VMEM((slots, part), BF),
            pltpu.VMEM((slots, hid), BF),
            pltpu.VMEM((slots, hid), BF),
            pltpu.VMEM((slots, hid), BF),
            pltpu.VMEM((width, hid), BF),
            pltpu.VMEM((width, hid), BF),
            pltpu.VMEM((hid, width), BF),
            pltpu.VMEM((tokens, width), BF),
            pltpu.VMEM((tokens, width), BF),
            pltpu.VMEM((tokens + 8, chan), F32),
            pltpu.VMEM((tokens, chan), F32),
            pltpu.VMEM((tokens, chan), BF),
            pltpu.VMEM((tokens + 8, chan), F32),
            pltpu.VMEM((experts // 2, 2, block, chan), BF),
            pltpu.VMEM((experts // 2, block, chan), BF),
            pltpu.VMEM((experts // 2, block, chan), BF),
            pltpu.VMEM((experts // 2, block, chan), BF),
            pltpu.VMEM((width, hid), F32),
            pltpu.VMEM((width, hid), F32),
            pltpu.VMEM((hid, width), F32),
            dma((4,)),
            dma((3,)),
        ]
        + [dma((8,))] * 12
        + [dma((2,))] * 6
        + [dma((5,))] * 2
        + [dma((8,))] * 2,
        compiler_params=pltpu.CompilerParams(
            collective_id=0, has_side_effects=True, vmem_limit_bytes=62 * 1024 * 1024
        ),
    )(choice, scale, cot, stream, gain, og, ig, ci, taps, wg, wu, wd, ow)


def finish_kernel(*refs):
    half = len(refs) // 2
    for given, out in zip(refs[:half], refs[half:]):
        out[...] = given[...].astype(out.dtype)


def finished_outputs(arrays, steps):
    types = [F32 if k > 3 else BF for k in range(len(arrays))]
    specs = [pl.BlockSpec((a.shape[0] // steps, a.shape[1]), lambda i: (i, 0)) for a in arrays]
    specs[4] = pl.BlockSpec(arrays[4].shape, lambda i: (0, 0))
    return pl.pallas_call(
        finish_kernel,
        name="finish",
        grid=(steps,),
        out_shape=[jax.ShapeDtypeStruct(a.shape, t) for a, t in zip(arrays, types)],
        in_specs=specs,
        out_specs=specs,
    )(*arrays)


def shards(
    cotangent,
    stream_in,
    norm_gain,
    out_gate,
    in_gate,
    conv_input,
    conv_taps,
    out_weight,
    expert_gate,
    expert_up,
    expert_down,
    expert_choice,
    route_scale,
):
    sp_size = lax.axis_size("sp")
    arrays = whole_step(
        expert_choice.T, route_scale.T, cotangent, stream_in, norm_gain[None], out_gate, in_gate, conv_input, conv_taps,
        expert_gate[0], expert_up[0], expert_down[0], out_weight, sp_size,
    )
    *others, grad_gate, grad_up, grad_down = finished_outputs(arrays, 4)
    return (*others, grad_gate[None], grad_up[None], grad_down[None])


def solution(mesh):
    placed = (
        P("sp", None),
        P("sp", None),
        P(),
        P("sp", "tp"),
        P("sp", "tp"),
        P("sp", "tp"),
        P(None, "tp"),
        P(None, "tp"),
        P("sp", None, "tp"),
        P("sp", None, "tp"),
        P("sp", "tp", None),
        P("sp", None),
        P("sp", None),
    )
    return jax.shard_map(
        shards,
        mesh=mesh,
        in_specs=placed,
        out_specs=(
            P("sp", "tp"),
            P("sp", "tp"),
            P("sp", "tp"),
            P("sp", "tp"),
            P("sp", "tp"),
            P("sp", None, "tp"),
            P("sp", None, "tp"),
            P("sp", "tp", None),
        ),
        check_vma=False,
    )
```

```python
import functools

import jax
import jax.numpy as jnp
from jax import lax
from jax.experimental import pallas as pl
from jax.experimental.pallas import tpu as pltpu
from jax.sharding import PartitionSpec as P

norm_eps = 1e-06
MESH = pl.DeviceIdType.MESH
CAP = 16
BF = jnp.bfloat16
F32 = jnp.float32


def rows_product(left, right):
    return lax.dot_general(left, right, (((0,), (0,)), ((), ())), preferred_element_type=F32)


def cols_product(left, right):
    return lax.dot_general(left, right, (((1,), (1,)), ((), ())), preferred_element_type=F32)


def product_of(left, right):
    return jnp.dot(left, right, preferred_element_type=F32)


def loop(low, high, body):
    def step(i, carry):
        body(i)
        return carry

    lax.fori_loop(low, high, step, 0)


def offset_of(t):
    half = lax.div(t + 1, 2)
    odd = lax.rem(t, 2)
    spread = odd * (1 + half) + (1 - odd) * (7 - half)
    return spread + 7 * lax.div(t + 7, 8) - 7 + 3 * lax.div(t, 6) - 7 * lax.div(t, 7)


def rows_at(index, count):
    return pl.ds(pl.multiple_of(index * count, count), count)


def step_kernel(
    plane, choice, scale, gain, taps, stream_hbm, cot_hbm, ig_hbm, ci_hbm, og_hbm, wg_hbm, wu_hbm, wd_hbm, ow_hbm,
    *refs,
):
    outs, refs = refs[:8], refs[8:]
    (
        stream, cot, ig, ci, og, wg, wu, wd, ow, inverse, normed, pick, weight, send_all, send_part, rows, partial, summand, far_in, far_sum, total, back,
        hidden, ggrad, ugrad, gate_out, up_out, down_out, tok, sgrad, extended, filtered, mixed, fgrad,
        owp, pair, psum, arrived, gate_sum, up_sum, down_sum,
        stream_out, og_out, ig_out, ci_out, ow_out,
        in_sem, out_sem,
        a_send, a_recv, half_recv, right_send, left_send, from_left, from_right,
        fright_send, fleft_send, ffrom_left, ffrom_right,
        rs_send, far_send, of_left_recv, of_right_recv, far_left_recv, far_right_recv, tright_send, tleft_send, tfrom_left, tfrom_right, tf_send, tf_recv, one_send, one_recv, pair_send, pair_recv,
    ) = refs
    me = lax.axis_index("sp")
    q = lax.axis_index("tp")
    right = lax.rem(q + 1, 4)
    left = lax.rem(q + 3, 4)
    z = lax.div(me, plane)
    place = lax.rem(me, plane)
    experts = 8 * plane
    span = plane * CAP
    tokens, width = cot.shape
    part = width // 4
    mine = rows_at(q, part)
    of_left = rows_at(left, part)
    of_right = rows_at(right, part)
    of_far = rows_at(lax.rem(q + 2, 4), part)
    my_slots = rows_at(me, CAP)

    def copy_to(src, dst, send, recv, sp, tp):
        pltpu.make_async_remote_copy(src, dst, send, recv, device_id=(sp, tp), device_id_type=MESH).start()

    def wait_for(ref, sem):
        pltpu.make_async_copy(ref, ref, sem).wait()

    def source_at(t):
        return lax.rem(z + 8 - offset_of(t), 8)

    def next_place(k):
        return lax.rem(place + k, plane)

    given = (stream_hbm, cot_hbm, ig_hbm, ci_hbm, og_hbm, wg_hbm, wu_hbm, wd_hbm, ow_hbm)
    held = (stream, cot, ig, ci, og, wg, wu, wd, ow)
    copies = [pltpu.make_async_copy(a, b, in_sem.at[n]) for n, (a, b) in enumerate(zip(given, held))]
    for copy in copies:
        copy.start()

    barrier = pltpu.get_barrier_semaphore()

    def greet(k):
        pl.semaphore_signal(barrier, inc=1, device_id=(lax.rem(me + k, experts), q), device_id_type=MESH)

    loop(1, experts, greet)

    def greet_row(k):
        pl.semaphore_signal(barrier, inc=1, device_id=(me, lax.rem(q + k, 4)), device_id_type=MESH)

    loop(1, 4, greet_row)

    first, second = choice[0:1, :], choice[1:2, :]
    ids = lax.broadcasted_iota(jnp.int32, (experts, tokens), 0)
    is_first, is_second = ids == first, ids == second
    named = jnp.where(is_first | is_second, 1.0, 0.0).astype(BF)
    before = jnp.where(
        lax.broadcasted_iota(jnp.int32, (tokens, tokens), 0) < lax.broadcasted_iota(jnp.int32, (tokens, tokens), 1), 1.0, 0.0
    ).astype(BF)
    earlier = product_of(named, before)
    slot_first = first * CAP + jnp.sum(jnp.where(is_first, earlier, 0.0), axis=0, keepdims=True).astype(jnp.int32)
    slot_second = second * CAP + jnp.sum(jnp.where(is_second, earlier, 0.0), axis=0, keepdims=True).astype(jnp.int32)

    def pick_rows(p):
        slots = lax.broadcasted_iota(jnp.int32, (span, tokens), 0) + p * span
        at_first, at_second = slots == slot_first, slots == slot_second
        pick[rows_at(p, span), :] = jnp.where(at_first | at_second, 1.0, 0.0).astype(BF)
        weight[rows_at(p, span), :] = jnp.sum(
            jnp.where(at_first, scale[0:1, :], 0.0) + jnp.where(at_second, scale[1:2, :], 0.0), axis=1, keepdims=True
        )

    loop(0, 8, pick_rows)

    copies[0].wait()

    def norm_rows(r):
        at = rows_at(r, 32)
        x = stream[at, :].astype(F32)
        inv = lax.rsqrt(jnp.mean(x * x, axis=-1, keepdims=True) + norm_eps)
        inverse[at, :] = inv
        normed[at, :] = ((x * inv) * gain[...]).astype(BF)

    loop(0, tokens // 32, norm_rows)

    copies[1].wait()

    def fill_quarter(t):
        at = rows_at(lax.rem(z + offset_of(t), 8), span)
        chosen = pick[at, :]
        send_part[t - 1, 0] = product_of(chosen, normed[:, mine]).astype(BF)
        send_part[t - 1, 1] = (product_of(chosen, cot[:, mine]) * weight[at, :]).astype(BF)

    loop(1, 6, fill_quarter)

    copies[2].wait()
    copies[3].wait()
    extended[8 : tokens + 8, :] = ig[...].astype(F32) * ci[...].astype(F32)

    @pl.when(me == 0)
    def _():
        extended[0:8, :] = jnp.zeros((8, part_of(extended)), F32)

    pl.semaphore_wait(barrier, experts + 2)

    @pl.when(me < experts - 1)
    def _():
        copy_to(extended.at[tokens : tokens + 8], extended.at[0:8], one_send.at[0], one_recv.at[0], me + 1, q)

    side = plane // 2

    def send_quarter(t):
        target = lax.rem(z + offset_of(t), 8)

        def one(k):
            turn = lax.div(k, side)
            block = lax.rem(lax.div(place, side) + turn, 2)
            to = block * side + lax.rem(place + k, side)
            copy_to(
                send_part.at[t - 1, :, rows_at(to, CAP), :], rows.at[:, my_slots, mine],
                a_send.at[t], half_recv.at[2 * t + turn], target * plane + to, q,
            )

        loop(0, plane, one)

    loop(1, 6, send_quarter)

    def turn_of(i):
        return i + 5 * lax.div(i + 1, 2)

    def fill_whole(i):
        at = rows_at(lax.rem(z + offset_of(turn_of(i)), 8), span)
        chosen = pick[at, :]
        send_all[i, 0] = product_of(chosen, normed[...]).astype(BF)
        send_all[i, 1] = (product_of(chosen, cot[...]) * weight[at, :]).astype(BF)

    loop(0, 3, fill_whole)
    own = rows_at(place, CAP)
    rows[0, my_slots, :] = send_all[0, 0, own, :]
    rows[1, my_slots, :] = send_all[0, 1, own, :]

    def send_whole(i):
        t = turn_of(i)
        target = lax.rem(z + offset_of(t), 8)

        def one(k):
            to = next_place(k)

            @pl.when(target * plane + to != me)
            def _():
                copy_to(
                    send_all.at[i, :, rows_at(to, CAP), :], rows.at[:, my_slots, :],
                    a_send.at[t], a_recv.at[t], target * plane + to, q,
                )

        loop(0, plane, one)


    send_whole(0)

    @pl.when(me > 0)
    def _():
        wait_for(extended.at[0:8], one_recv.at[0])

    copies[4].wait()
    now = (
        taps[0:1, :] * extended[8 : tokens + 8, :]
        + taps[1:2, :] * extended[7 : tokens + 7, :]
        + taps[2:3, :] * extended[6 : tokens + 6, :]
    )
    filtered[...] = now
    mixed[...] = (og[...].astype(F32) * now).astype(BF)
    chunk = min(256, width)

    def clear(m):
        cols = rows_at(m, chunk)
        gate_sum[cols, :] = jnp.zeros((chunk, part_of(gate_sum)), F32)
        up_sum[cols, :] = jnp.zeros((chunk, part_of(up_sum)), F32)
        down_sum[:, cols] = jnp.zeros((down_sum.shape[0], chunk), F32)

    loop(0, width // chunk, clear)
    for copy in copies[5:]:
        copy.wait()

    def add_grads(at):
        def one(m):
            cols = rows_at(m, chunk)
            here = rows[0, at, cols]
            gate_sum[cols, :] += rows_product(here, ggrad[at, :])
            up_sum[cols, :] += rows_product(here, ugrad[at, :])
            down_sum[:, cols] += rows_product(hidden[at, :], rows[1, at, cols])

        loop(0, width // chunk, one)

    def halves_at(t):
        source = source_at(t)
        return rows_at(2 * source, span // 2), rows_at(2 * source + 1, span // 2), source

    def pass_sum(t):
        upper, lower, source = halves_at(t)
        held_at = rows_at(source, span // 2)
        wait_for(far_in.at[0, held_at, :], far_left_recv.at[t])
        far_sum[0, held_at, :] = (partial[upper, of_right].astype(F32) + far_in[0, held_at, :].astype(F32)).astype(BF)
        copy_to(far_sum.at[0, held_at, :], summand.at[0, upper, :], rs_send.at[t], of_left_recv.at[t], me, right)
        wait_for(far_in.at[1, held_at, :], far_right_recv.at[t])
        far_sum[1, held_at, :] = (partial[lower, of_left].astype(F32) + far_in[1, held_at, :].astype(F32)).astype(BF)
        copy_to(far_sum.at[1, held_at, :], summand.at[1, lower, :], rs_send.at[t], of_right_recv.at[t], me, left)

    def step(i):
        @pl.when((i >= 1) & (i < 6))
        def _():
            for turn in range(2):
                block = lax.rem(lax.div(place, side) + turn, 2)
                piece = rows.at[:, rows_at(2 * source_at(i) + block, span // 2), mine]
                wait_for(piece, half_recv.at[2 * i + turn])
                copy_to(piece, piece, right_send.at[i], from_left.at[i], me, right)
                copy_to(piece, piece, left_send.at[i], from_right.at[i], me, left)

        @pl.when(i == 3)
        def _():
            send_whole(1)
            send_whole(2)

        @pl.when((i >= 2) & (i < 7))
        def _():
            t = i - 1
            at = rows_at(source_at(t), span)
            wait_for(rows.at[:, at, of_left], from_left.at[t])
            half = rows.at[0, at, of_left]
            copy_to(half, half, fright_send.at[t], ffrom_left.at[t], me, right)
            wait_for(rows.at[:, at, of_right], from_right.at[t])
            half = rows.at[1, at, of_right]
            copy_to(half, half, fleft_send.at[t], ffrom_right.at[t], me, left)

        @pl.when((i >= 3) & (i < 8))
        def _():
            pass_sum(i - 3)

        @pl.when((i >= 2) & (i < 10))
        def _():
            t = i - 2
            at = rows_at(source_at(t), span)

            @pl.when((t >= 1) & (t < 6))
            def _():
                wait_for(rows.at[0, at, of_far], ffrom_left.at[t])
                wait_for(rows.at[1, at, of_far], ffrom_right.at[t])

            @pl.when(t == 0)
            def _():
                if plane > 1:
                    wait_for(rows.at[:, pl.ds(0, (plane - 1) * CAP), :], a_recv.at[0])

            @pl.when(t >= 6)
            def _():
                wait_for(rows.at[:, at, :], a_recv.at[t])

            here = rows[0, at, :]
            gate_pre = product_of(here, wg[...])
            up_pre = product_of(here, wu[...])
            hidden_grad = cols_product(rows[1, at, :], wd[...])
            sigmoid_gate = jax.nn.sigmoid(gate_pre)
            silu_gate = gate_pre * sigmoid_gate
            hidden[at, :] = (silu_gate * up_pre).astype(BF)
            gate_grad = (hidden_grad * up_pre * sigmoid_gate * (1.0 + gate_pre * (1.0 - sigmoid_gate))).astype(BF)
            up_grad = (hidden_grad * silu_gate).astype(BF)
            ggrad[at, :] = gate_grad
            ugrad[at, :] = up_grad
            partial[at, :] = (cols_product(gate_grad, wg[...]) + cols_product(up_grad, wu[...])).astype(BF)

            upper, lower, source = halves_at(t)
            held_at = rows_at(source, span // 2)
            copy_to(partial.at[upper, of_far], far_in.at[0, held_at, :], far_send.at[t], far_left_recv.at[t], me, right)
            copy_to(partial.at[lower, of_far], far_in.at[1, held_at, :], far_send.at[t], far_right_recv.at[t], me, left)
            copy_to(partial.at[lower, of_right], summand.at[0, lower, :], rs_send.at[t], of_left_recv.at[t], me, right)
            copy_to(partial.at[upper, of_left], summand.at[1, upper, :], rs_send.at[t], of_right_recv.at[t], me, left)

            @pl.when(t < 6)
            def _():
                add_grads(at)

        @pl.when((i >= 8) & (i < 11))
        def _():
            pass_sum(i - 3)

        @pl.when(i >= 4)
        def _():
            t = i - 4
            source = source_at(t)
            at = rows_at(source, span)
            wait_for(summand.at[0, at, :], of_left_recv.at[t])
            wait_for(summand.at[1, at, :], of_right_recv.at[t])
            added = partial[at, mine].astype(F32) + summand[0, at, :].astype(F32) + summand[1, at, :].astype(F32)
            total[at, :] = added.astype(BF)

            def one(k):
                to = source * plane + next_place(k)

                @pl.when(to != me)
                def _():
                    copy_to(total.at[rows_at(to, CAP), :], back.at[my_slots, :], one_send.at[1], one_recv.at[1], to, q)

            loop(0, plane, one)

    loop(1, 12, step)
    back[my_slots, :] = total[my_slots, :]

    def late_grads(t):
        add_grads(rows_at(source_at(t), span))

    loop(6, 7, late_grads)

    wait_for(back.at[pl.ds(0, (experts - 1) * CAP), :], one_recv.at[1])
    tok[:, mine] = rows_product(pick[...], back[...]).astype(BF)
    half = tokens // 2
    low, high = pl.ds(0, half), pl.ds(half, half)
    for h, at in ((0, low), (1, high)):
        copy_to(tok.at[at, mine], tok.at[at, mine], tright_send.at[h], tfrom_left.at[h], me, right)
    for h, at in ((1, high), (0, low)):
        copy_to(tok.at[at, mine], tok.at[at, mine], tleft_send.at[h], tfrom_right.at[h], me, left)
    loop(7, 8, late_grads)
    wait_for(tok.at[low, of_left], tfrom_left.at[0])
    copy_to(tok.at[low, of_left], tok.at[low, of_left], tf_send.at[0], tf_recv.at[0], me, right)
    wait_for(tok.at[high, of_right], tfrom_right.at[1])
    copy_to(tok.at[high, of_right], tok.at[high, of_right], tf_send.at[1], tf_recv.at[1], me, left)
    def narrow(m):
        cols = rows_at(m, chunk)
        gate_out[cols, :] = gate_sum[cols, :].astype(BF)
        up_out[cols, :] = up_sum[cols, :].astype(BF)
        down_out[:, cols] = down_sum[:, cols].astype(BF)

    loop(0, width // chunk, narrow)
    ready = (stream_out, og_out, ig_out, ci_out, ow_out, gate_out, up_out, down_out)
    finished = [pltpu.make_async_copy(a, b, out_sem.at[n]) for n, (a, b) in enumerate(zip(ready, outs))]
    for copy in finished[5:]:
        copy.start()

    wait_for(tok.at[high, of_left], tfrom_left.at[1])
    wait_for(tok.at[low, of_right], tfrom_right.at[0])
    wait_for(tok.at[low, of_far], tf_recv.at[0])
    wait_for(tok.at[high, of_far], tf_recv.at[1])

    def stream_rows(r):
        at = rows_at(r, 16)
        inv = inverse[at, :]
        unit = stream[at, :].astype(F32) * inv
        unit_grad = tok[at, :].astype(F32) * gain[...]
        along = jnp.mean(unit * unit_grad, axis=-1, keepdims=True)
        sgrad[at, :] = (cot[at, :].astype(F32) + inv * (unit_grad - unit * along)).astype(BF)

    loop(0, tokens // 16, stream_rows)

    block = width // experts
    pairs = experts // 2
    core = lax.rem(me, 2)
    here = lax.div(me, 2)
    groups = plane // 2
    cut = plane * block

    def plane_of(j):
        half = lax.div(j + 1, 2)
        return lax.rem(z + 4 + half - 2 * half * lax.rem(j, 2), 8)

    def out_rows(j):
        at = plane_of(j)
        found = rows_product(sgrad[:, rows_at(at, cut)], mixed[...]).astype(BF)
        of_plane = rows_at(at, groups)
        owp[of_plane] = found.reshape(groups, 2, block, found.shape[-1])
        copy_to(owp.at[of_plane, 1 - core], pair.at[of_plane], pair_send.at[j], pair_recv.at[j], me + 1 - 2 * core, q)

    loop(0, 8, out_rows)

    def pair_sum(j):
        at = plane_of(j)
        of_plane = rows_at(at, groups)
        wait_for(pair.at[of_plane], pair_recv.at[j])
        psum[of_plane] = (owp[of_plane, core].astype(F32) + pair[of_plane].astype(F32)).astype(BF)

        def send_sum(k):
            to = at * groups + lax.rem(here + k, groups)

            @pl.when(to != here)
            def _():
                copy_to(psum.at[to], arrived.at[here], one_send.at[4], one_recv.at[4], 2 * to + core, q)

        loop(0, groups, send_sum)

    loop(0, 8, pair_sum)
    arrived[here] = psum[here]

    mixed_grad = product_of(sgrad[...], ow[...])
    fgrad[0:tokens, :] = mixed_grad * og[...].astype(F32)

    @pl.when(me > 0)
    def _():
        copy_to(fgrad.at[0:8], fgrad.at[tokens : tokens + 8], one_send.at[3], one_recv.at[3], me - 1, q)

    @pl.when(me == experts - 1)
    def _():
        fgrad[tokens : tokens + 8, :] = jnp.zeros((8, part_of(fgrad)), F32)

    og_out[...] = (mixed_grad * filtered[...]).astype(BF)
    finished[1].start()
    stream_out[...] = sgrad[:, mine]
    finished[0].start()

    @pl.when(me < experts - 1)
    def _():
        wait_for(fgrad.at[tokens : tokens + 8], one_recv.at[3])

    product_grad = (
        taps[0:1, :] * fgrad[0:tokens, :] + taps[1:2, :] * fgrad[1 : tokens + 1, :] + taps[2:3, :] * fgrad[2 : tokens + 2, :]
    )
    ig_out[...] = (product_grad * ci[...].astype(F32)).astype(BF)
    ci_out[...] = (product_grad * ig[...].astype(F32)).astype(BF)
    finished[2].start()
    finished[3].start()

    def sent_rows(t):
        @pl.when((t >= 1) & (t < 6))
        def _():
            piece = rows.at[:, rows_at(0, span), mine]
            wait_for(piece, a_send.at[t])
            wait_for(piece, right_send.at[t])
            wait_for(piece, left_send.at[t])
            wait_for(rows.at[0, rows_at(0, span), mine], fright_send.at[t])
            wait_for(rows.at[0, rows_at(0, span), mine], fleft_send.at[t])

        @pl.when(t == 0)
        def _():
            if plane > 1:
                wait_for(rows.at[:, pl.ds(0, (plane - 1) * CAP), :], a_send.at[0])

        @pl.when(t >= 6)
        def _():
            wait_for(rows.at[:, rows_at(0, span), :], a_send.at[t])

        wait_for(summand.at[:, rows_at(0, span), :], rs_send.at[t])
        wait_for(summand.at[0, rows_at(0, span), :], far_send.at[t])

    loop(0, 8, sent_rows)
    wait_for(back.at[pl.ds(0, (experts - 1) * CAP), :], one_send.at[1])
    for h in range(2):
        wait_for(tok.at[low, mine], tright_send.at[h])
        wait_for(tok.at[low, mine], tleft_send.at[h])
        wait_for(tok.at[low, mine], tf_send.at[h])

    def pair_sent(j):
        wait_for(pair.at[pl.ds(0, groups)], pair_send.at[j])

    loop(0, 8, pair_sent)

    @pl.when(me < experts - 1)
    def _():
        wait_for(extended.at[0:8], one_send.at[0])

    @pl.when(me > 0)
    def _():
        wait_for(fgrad.at[0:8], one_send.at[3])

    wait_for(arrived.at[pl.ds(0, pairs - 1)], one_recv.at[4])
    added = arrived[0].astype(F32)
    for p in range(1, pairs):
        added = added + arrived[p].astype(F32)
    ow_out[...] = added
    finished[4].start()
    for copy in finished:
        copy.wait()
    wait_for(arrived.at[pl.ds(0, pairs - 1)], one_send.at[4])


def part_of(ref):
    return ref.shape[-1]


def whole_step(choice, scale, gain, taps, stream, cot, ig, ci, og, wg, wu, wd, ow, experts):
    tokens, width = cot.shape
    part = width // 4
    slots = experts * CAP
    plane = experts // 8
    hid = wg.shape[1]
    chan = og.shape[1]
    block = width // experts
    vm = pl.BlockSpec(memory_space=pltpu.VMEM)
    hbm = pl.BlockSpec(memory_space=pltpu.HBM)
    dma = pltpu.SemaphoreType.DMA
    return pl.pallas_call(
        functools.partial(step_kernel, plane),
        name="experts",
        out_shape=(
            jax.ShapeDtypeStruct((tokens, part), BF),
            jax.ShapeDtypeStruct((tokens, chan), BF),
            jax.ShapeDtypeStruct((tokens, chan), BF),
            jax.ShapeDtypeStruct((tokens, chan), BF),
            jax.ShapeDtypeStruct((block, chan), F32),
            jax.ShapeDtypeStruct((width, hid), BF),
            jax.ShapeDtypeStruct((width, hid), BF),
            jax.ShapeDtypeStruct((hid, width), BF),
        ),
        in_specs=[vm] * 4 + [hbm] * 9,
        out_specs=(hbm,) * 8,
        scratch_shapes=[
            pltpu.VMEM((tokens, width), BF),
            pltpu.VMEM((tokens, width), BF),
            pltpu.VMEM((tokens, chan), BF),
            pltpu.VMEM((tokens, chan), BF),
            pltpu.VMEM((tokens, chan), BF),
            pltpu.VMEM((width, hid), BF),
            pltpu.VMEM((width, hid), BF),
            pltpu.VMEM((hid, width), BF),
            pltpu.VMEM((width, chan), BF),
            pltpu.VMEM((tokens, 1), F32),
            pltpu.VMEM((tokens, width), BF),
            pltpu.VMEM((slots, tokens), BF),
            pltpu.VMEM((slots, 1), F32),
            pltpu.VMEM((3, 2, plane * CAP, width), BF),
            pltpu.VMEM((5, 2, plane * CAP, part), BF),
            pltpu.VMEM((2, slots, width), BF),
            pltpu.VMEM((slots, width), BF),
            pltpu.VMEM((2, slots, part), BF),
            pltpu.VMEM((2, slots // 2, part), BF),
            pltpu.VMEM((2, slots // 2, part), BF),
            pltpu.VMEM((slots, part), BF),
            pltpu.VMEM((slots, part), BF),
            pltpu.VMEM((slots, hid), BF),
            pltpu.VMEM((slots, hid), BF),
            pltpu.VMEM((slots, hid), BF),
            pltpu.VMEM((width, hid), BF),
            pltpu.VMEM((width, hid), BF),
            pltpu.VMEM((hid, width), BF),
            pltpu.VMEM((tokens, width), BF),
            pltpu.VMEM((tokens, width), BF),
            pltpu.VMEM((tokens + 8, chan), F32),
            pltpu.VMEM((tokens, chan), F32),
            pltpu.VMEM((tokens, chan), BF),
            pltpu.VMEM((tokens + 8, chan), F32),
            pltpu.VMEM((experts // 2, 2, block, chan), BF),
            pltpu.VMEM((experts // 2, block, chan), BF),
            pltpu.VMEM((experts // 2, block, chan), BF),
            pltpu.VMEM((experts // 2, block, chan), BF),
            pltpu.VMEM((width, hid), F32),
            pltpu.VMEM((width, hid), F32),
            pltpu.VMEM((hid, width), F32),
            pltpu.VMEM((tokens, part), BF),
            pltpu.VMEM((tokens, chan), BF),
            pltpu.VMEM((tokens, chan), BF),
            pltpu.VMEM((tokens, chan), BF),
            pltpu.VMEM((block, chan), F32),
            dma((9,)),
            dma((8,)),
        ]
        + [dma((8,))] * 2
        + [dma((16,))]
        + [dma((8,))] * 14
        + [dma((2,))] * 6
        + [dma((5,))] * 2
        + [dma((8,))] * 2,
        compiler_params=pltpu.CompilerParams(
            collective_id=0, has_side_effects=True, vmem_limit_bytes=62 * 1024 * 1024
        ),
    )(choice, scale, gain, taps, stream, cot, ig, ci, og, wg, wu, wd, ow)


def finish_kernel(*refs):
    half = len(refs) // 2
    for given, out in zip(refs[:half], refs[half:]):
        out[...] = given[...].astype(out.dtype)


def finished_outputs(arrays, steps):
    types = [F32 if k > 3 else BF for k in range(len(arrays))]
    specs = [pl.BlockSpec((a.shape[0] // steps, a.shape[1]), lambda i: (i, 0)) for a in arrays]
    specs[4] = pl.BlockSpec(arrays[4].shape, lambda i: (0, 0))
    return pl.pallas_call(
        finish_kernel,
        name="finish",
        grid=(steps,),
        out_shape=[jax.ShapeDtypeStruct(a.shape, t) for a, t in zip(arrays, types)],
        in_specs=specs,
        out_specs=specs,
    )(*arrays)


def shards(
    cotangent,
    stream_in,
    norm_gain,
    out_gate,
    in_gate,
    conv_input,
    conv_taps,
    out_weight,
    expert_gate,
    expert_up,
    expert_down,
    expert_choice,
    route_scale,
):
    sp_size = lax.axis_size("sp")
    arrays = whole_step(
        expert_choice.T, route_scale.T, norm_gain[None], conv_taps, stream_in, cotangent, in_gate, conv_input, out_gate,
        expert_gate[0], expert_up[0], expert_down[0], out_weight, sp_size,
    )
    *others, grad_gate, grad_up, grad_down = finished_outputs(arrays, 4)
    return (*others, grad_gate[None], grad_up[None], grad_down[None])


def solution(mesh):
    placed = (
        P("sp", None),
        P("sp", None),
        P(),
        P("sp", "tp"),
        P("sp", "tp"),
        P("sp", "tp"),
        P(None, "tp"),
        P(None, "tp"),
        P("sp", None, "tp"),
        P("sp", None, "tp"),
        P("sp", "tp", None),
        P("sp", None),
        P("sp", None),
    )
    return jax.shard_map(
        shards,
        mesh=mesh,
        in_specs=placed,
        out_specs=(
            P("sp", "tp"),
            P("sp", "tp"),
            P("sp", "tp"),
            P("sp", "tp"),
            P("sp", "tp"),
            P("sp", None, "tp"),
            P("sp", None, "tp"),
            P("sp", "tp", None),
        ),
        check_vma=False,
    )
```

```python
import functools

import jax
import jax.numpy as jnp
from jax import lax
from jax.experimental import pallas as pl
from jax.experimental.pallas import tpu as pltpu
from jax.sharding import PartitionSpec as P

norm_eps = 1e-06
MESH = pl.DeviceIdType.MESH
CAP = 16
BF = jnp.bfloat16
F32 = jnp.float32


def rows_product(left, right):
    return lax.dot_general(left, right, (((0,), (0,)), ((), ())), preferred_element_type=F32)


def cols_product(left, right):
    return lax.dot_general(left, right, (((1,), (1,)), ((), ())), preferred_element_type=F32)


def product_of(left, right):
    return jnp.dot(left, right, preferred_element_type=F32)


def loop(low, high, body):
    def step(i, carry):
        body(i)
        return carry

    lax.fori_loop(low, high, step, 0)


def offset_of(t):
    half = lax.div(t + 1, 2)
    odd = lax.rem(t, 2)
    spread = odd * (1 + half) + (1 - odd) * (7 - half)
    return spread + 7 * lax.div(t + 7, 8) - 7 + 3 * lax.div(t, 6) - 7 * lax.div(t, 7)


def rows_at(index, count):
    return pl.ds(pl.multiple_of(index * count, count), count)


def step_kernel(
    plane, choice, scale, gain, taps, stream_hbm, cot_hbm, ig_hbm, ci_hbm, og_hbm, wg_hbm, wu_hbm, wd_hbm, ow_hbm,
    *refs,
):
    outs, refs = refs[:8], refs[8:]
    (
        stream, cot, ig, ci, og, wg, wu, wd, ow, inverse, normed, pick, weight, send_all, send_part, rows, partial, summand, far_in, far_sum, total, back,
        hidden, ggrad, ugrad, gate_out, up_out, down_out, tok, sgrad, extended, filtered, mixed, fgrad,
        owp, pair, psum, row_in, row_total, arrived, gate_sum, up_sum, down_sum,
        stream_out, og_out, ig_out, ci_out, ow_out,
        in_sem, out_sem,
        a_send, a_recv, half_recv, right_send, left_send, from_left, from_right,
        fright_send, fleft_send, ffrom_left, ffrom_right,
        rs_send, far_send, of_left_recv, of_right_recv, far_left_recv, far_right_recv, tright_send, tleft_send, tfrom_left, tfrom_right, tf_send, tf_recv, one_send, one_recv, pair_send, pair_recv, row_send, row_recv,
    ) = refs
    me = lax.axis_index("sp")
    q = lax.axis_index("tp")
    right = lax.rem(q + 1, 4)
    left = lax.rem(q + 3, 4)
    z = lax.div(me, plane)
    place = lax.rem(me, plane)
    experts = 8 * plane
    span = plane * CAP
    tokens, width = cot.shape
    part = width // 4
    mine = rows_at(q, part)
    of_left = rows_at(left, part)
    of_right = rows_at(right, part)
    of_far = rows_at(lax.rem(q + 2, 4), part)
    my_slots = rows_at(me, CAP)

    def copy_to(src, dst, send, recv, sp, tp):
        pltpu.make_async_remote_copy(src, dst, send, recv, device_id=(sp, tp), device_id_type=MESH).start()

    def wait_for(ref, sem):
        pltpu.make_async_copy(ref, ref, sem).wait()

    def source_at(t):
        return lax.rem(z + 8 - offset_of(t), 8)

    def next_place(k):
        return lax.rem(place + k, plane)

    given = (stream_hbm, cot_hbm, ig_hbm, ci_hbm, og_hbm, wg_hbm, wu_hbm, wd_hbm, ow_hbm)
    held = (stream, cot, ig, ci, og, wg, wu, wd, ow)
    copies = [pltpu.make_async_copy(a, b, in_sem.at[n]) for n, (a, b) in enumerate(zip(given, held))]
    for copy in copies:
        copy.start()

    barrier = pltpu.get_barrier_semaphore()

    def greet(k):
        pl.semaphore_signal(barrier, inc=1, device_id=(lax.rem(me + k, experts), q), device_id_type=MESH)

    loop(1, experts, greet)

    def greet_row(k):
        pl.semaphore_signal(barrier, inc=1, device_id=(me, lax.rem(q + k, 4)), device_id_type=MESH)

    loop(1, 4, greet_row)

    first, second = choice[0:1, :], choice[1:2, :]
    ids = lax.broadcasted_iota(jnp.int32, (experts, tokens), 0)
    is_first, is_second = ids == first, ids == second
    named = jnp.where(is_first | is_second, 1.0, 0.0).astype(BF)
    before = jnp.where(
        lax.broadcasted_iota(jnp.int32, (tokens, tokens), 0) < lax.broadcasted_iota(jnp.int32, (tokens, tokens), 1), 1.0, 0.0
    ).astype(BF)
    earlier = product_of(named, before)
    slot_first = first * CAP + jnp.sum(jnp.where(is_first, earlier, 0.0), axis=0, keepdims=True).astype(jnp.int32)
    slot_second = second * CAP + jnp.sum(jnp.where(is_second, earlier, 0.0), axis=0, keepdims=True).astype(jnp.int32)

    def pick_rows(p):
        slots = lax.broadcasted_iota(jnp.int32, (span, tokens), 0) + p * span
        at_first, at_second = slots == slot_first, slots == slot_second
        pick[rows_at(p, span), :] = jnp.where(at_first | at_second, 1.0, 0.0).astype(BF)
        weight[rows_at(p, span), :] = jnp.sum(
            jnp.where(at_first, scale[0:1, :], 0.0) + jnp.where(at_second, scale[1:2, :], 0.0), axis=1, keepdims=True
        )

    loop(0, 8, pick_rows)

    copies[0].wait()

    def norm_rows(r):
        at = rows_at(r, 32)
        x = stream[at, :].astype(F32)
        inv = lax.rsqrt(jnp.mean(x * x, axis=-1, keepdims=True) + norm_eps)
        inverse[at, :] = inv
        normed[at, :] = ((x * inv) * gain[...]).astype(BF)

    loop(0, tokens // 32, norm_rows)

    copies[1].wait()

    def fill_quarter(t):
        at = rows_at(lax.rem(z + offset_of(t), 8), span)
        chosen = pick[at, :]
        send_part[t - 1, 0] = product_of(chosen, normed[:, mine]).astype(BF)
        send_part[t - 1, 1] = (product_of(chosen, cot[:, mine]) * weight[at, :]).astype(BF)

    loop(1, 6, fill_quarter)

    copies[2].wait()
    copies[3].wait()
    extended[8 : tokens + 8, :] = ig[...].astype(F32) * ci[...].astype(F32)

    @pl.when(me == 0)
    def _():
        extended[0:8, :] = jnp.zeros((8, part_of(extended)), F32)

    pl.semaphore_wait(barrier, experts + 2)

    @pl.when(me < experts - 1)
    def _():
        copy_to(extended.at[tokens : tokens + 8], extended.at[0:8], one_send.at[0], one_recv.at[0], me + 1, q)

    side = plane // 2

    def send_quarter(t):
        target = lax.rem(z + offset_of(t), 8)

        def one(k):
            turn = lax.div(k, side)
            block = lax.rem(lax.div(place, side) + turn, 2)
            to = block * side + lax.rem(place + k, side)
            copy_to(
                send_part.at[t - 1, :, rows_at(to, CAP), :], rows.at[:, my_slots, mine],
                a_send.at[t], half_recv.at[2 * t + turn], target * plane + to, q,
            )

        loop(0, plane, one)

    loop(1, 6, send_quarter)

    def turn_of(i):
        return i + 5 * lax.div(i + 1, 2)

    def fill_whole(i):
        at = rows_at(lax.rem(z + offset_of(turn_of(i)), 8), span)
        chosen = pick[at, :]
        send_all[i, 0] = product_of(chosen, normed[...]).astype(BF)
        send_all[i, 1] = (product_of(chosen, cot[...]) * weight[at, :]).astype(BF)

    loop(0, 3, fill_whole)
    own = rows_at(place, CAP)
    rows[0, my_slots, :] = send_all[0, 0, own, :]
    rows[1, my_slots, :] = send_all[0, 1, own, :]

    def send_whole(i):
        t = turn_of(i)
        target = lax.rem(z + offset_of(t), 8)

        def one(k):
            to = next_place(k)

            @pl.when(target * plane + to != me)
            def _():
                copy_to(
                    send_all.at[i, :, rows_at(to, CAP), :], rows.at[:, my_slots, :],
                    a_send.at[t], a_recv.at[t], target * plane + to, q,
                )

        loop(0, plane, one)


    send_whole(0)

    @pl.when(me > 0)
    def _():
        wait_for(extended.at[0:8], one_recv.at[0])

    copies[4].wait()
    now = (
        taps[0:1, :] * extended[8 : tokens + 8, :]
        + taps[1:2, :] * extended[7 : tokens + 7, :]
        + taps[2:3, :] * extended[6 : tokens + 6, :]
    )
    filtered[...] = now
    mixed[...] = (og[...].astype(F32) * now).astype(BF)
    chunk = min(256, width)

    def clear(m):
        cols = rows_at(m, chunk)
        gate_sum[cols, :] = jnp.zeros((chunk, part_of(gate_sum)), F32)
        up_sum[cols, :] = jnp.zeros((chunk, part_of(up_sum)), F32)
        down_sum[:, cols] = jnp.zeros((down_sum.shape[0], chunk), F32)

    loop(0, width // chunk, clear)
    for copy in copies[5:]:
        copy.wait()

    def add_grads(at):
        def one(m):
            cols = rows_at(m, chunk)
            here = rows[0, at, cols]
            gate_sum[cols, :] += rows_product(here, ggrad[at, :])
            up_sum[cols, :] += rows_product(here, ugrad[at, :])
            down_sum[:, cols] += rows_product(hidden[at, :], rows[1, at, cols])

        loop(0, width // chunk, one)

    def halves_at(t):
        source = source_at(t)
        return rows_at(2 * source, span // 2), rows_at(2 * source + 1, span // 2), source

    def pass_sum(t):
        upper, lower, source = halves_at(t)
        held_at = rows_at(source, span // 2)
        wait_for(far_in.at[0, held_at, :], far_left_recv.at[t])
        far_sum[0, held_at, :] = (partial[upper, of_right].astype(F32) + far_in[0, held_at, :].astype(F32)).astype(BF)
        copy_to(far_sum.at[0, held_at, :], summand.at[0, upper, :], rs_send.at[t], of_left_recv.at[t], me, right)
        wait_for(far_in.at[1, held_at, :], far_right_recv.at[t])
        far_sum[1, held_at, :] = (partial[lower, of_left].astype(F32) + far_in[1, held_at, :].astype(F32)).astype(BF)
        copy_to(far_sum.at[1, held_at, :], summand.at[1, lower, :], rs_send.at[t], of_right_recv.at[t], me, left)

    def step(i):
        @pl.when((i >= 1) & (i < 6))
        def _():
            for turn in range(2):
                block = lax.rem(lax.div(place, side) + turn, 2)
                piece = rows.at[:, rows_at(2 * source_at(i) + block, span // 2), mine]
                wait_for(piece, half_recv.at[2 * i + turn])
                copy_to(piece, piece, right_send.at[i], from_left.at[i], me, right)
                copy_to(piece, piece, left_send.at[i], from_right.at[i], me, left)

        @pl.when(i == 3)
        def _():
            send_whole(1)
            send_whole(2)

        @pl.when((i >= 2) & (i < 7))
        def _():
            t = i - 1
            at = rows_at(source_at(t), span)
            wait_for(rows.at[:, at, of_left], from_left.at[t])
            half = rows.at[0, at, of_left]
            copy_to(half, half, fright_send.at[t], ffrom_left.at[t], me, right)
            wait_for(rows.at[:, at, of_right], from_right.at[t])
            half = rows.at[1, at, of_right]
            copy_to(half, half, fleft_send.at[t], ffrom_right.at[t], me, left)

        @pl.when((i >= 3) & (i < 8))
        def _():
            pass_sum(i - 3)

        @pl.when((i >= 2) & (i < 10))
        def _():
            t = i - 2
            at = rows_at(source_at(t), span)

            @pl.when((t >= 1) & (t < 6))
            def _():
                wait_for(rows.at[0, at, of_far], ffrom_left.at[t])
                wait_for(rows.at[1, at, of_far], ffrom_right.at[t])

            @pl.when(t == 0)
            def _():
                if plane > 1:
                    wait_for(rows.at[:, pl.ds(0, (plane - 1) * CAP), :], a_recv.at[0])

            @pl.when(t >= 6)
            def _():
                wait_for(rows.at[:, at, :], a_recv.at[t])

            here = rows[0, at, :]
            gate_pre = product_of(here, wg[...])
            up_pre = product_of(here, wu[...])
            hidden_grad = cols_product(rows[1, at, :], wd[...])
            sigmoid_gate = jax.nn.sigmoid(gate_pre)
            silu_gate = gate_pre * sigmoid_gate
            hidden[at, :] = (silu_gate * up_pre).astype(BF)
            gate_grad = (hidden_grad * up_pre * sigmoid_gate * (1.0 + gate_pre * (1.0 - sigmoid_gate))).astype(BF)
            up_grad = (hidden_grad * silu_gate).astype(BF)
            ggrad[at, :] = gate_grad
            ugrad[at, :] = up_grad
            partial[at, :] = (cols_product(gate_grad, wg[...]) + cols_product(up_grad, wu[...])).astype(BF)

            upper, lower, source = halves_at(t)
            held_at = rows_at(source, span // 2)
            copy_to(partial.at[upper, of_far], far_in.at[0, held_at, :], far_send.at[t], far_left_recv.at[t], me, right)
            copy_to(partial.at[lower, of_far], far_in.at[1, held_at, :], far_send.at[t], far_right_recv.at[t], me, left)
            copy_to(partial.at[lower, of_right], summand.at[0, lower, :], rs_send.at[t], of_left_recv.at[t], me, right)
            copy_to(partial.at[upper, of_left], summand.at[1, upper, :], rs_send.at[t], of_right_recv.at[t], me, left)

            @pl.when(t < 6)
            def _():
                add_grads(at)

        @pl.when((i >= 8) & (i < 11))
        def _():
            pass_sum(i - 3)

        @pl.when(i >= 4)
        def _():
            t = i - 4
            source = source_at(t)
            at = rows_at(source, span)
            wait_for(summand.at[0, at, :], of_left_recv.at[t])
            wait_for(summand.at[1, at, :], of_right_recv.at[t])
            added = partial[at, mine].astype(F32) + summand[0, at, :].astype(F32) + summand[1, at, :].astype(F32)
            total[at, :] = added.astype(BF)

            def one(k):
                to = source * plane + next_place(k)

                @pl.when(to != me)
                def _():
                    copy_to(total.at[rows_at(to, CAP), :], back.at[my_slots, :], one_send.at[1], one_recv.at[1], to, q)

            loop(0, plane, one)

    loop(1, 12, step)
    back[my_slots, :] = total[my_slots, :]

    def late_grads(t):
        add_grads(rows_at(source_at(t), span))

    loop(6, 7, late_grads)

    wait_for(back.at[pl.ds(0, (experts - 1) * CAP), :], one_recv.at[1])
    tok[:, mine] = rows_product(pick[...], back[...]).astype(BF)
    half = tokens // 2
    low, high = pl.ds(0, half), pl.ds(half, half)
    for h, at in ((0, low), (1, high)):
        copy_to(tok.at[at, mine], tok.at[at, mine], tright_send.at[h], tfrom_left.at[h], me, right)
    for h, at in ((1, high), (0, low)):
        copy_to(tok.at[at, mine], tok.at[at, mine], tleft_send.at[h], tfrom_right.at[h], me, left)
    loop(7, 8, late_grads)
    wait_for(tok.at[low, of_left], tfrom_left.at[0])
    copy_to(tok.at[low, of_left], tok.at[low, of_left], tf_send.at[0], tf_recv.at[0], me, right)
    wait_for(tok.at[high, of_right], tfrom_right.at[1])
    copy_to(tok.at[high, of_right], tok.at[high, of_right], tf_send.at[1], tf_recv.at[1], me, left)
    def narrow(m):
        cols = rows_at(m, chunk)
        gate_out[cols, :] = gate_sum[cols, :].astype(BF)
        up_out[cols, :] = up_sum[cols, :].astype(BF)
        down_out[:, cols] = down_sum[:, cols].astype(BF)

    loop(0, width // chunk, narrow)
    ready = (stream_out, og_out, ig_out, ci_out, ow_out, gate_out, up_out, down_out)
    finished = [pltpu.make_async_copy(a, b, out_sem.at[n]) for n, (a, b) in enumerate(zip(ready, outs))]
    for copy in finished[5:]:
        copy.start()

    wait_for(tok.at[high, of_left], tfrom_left.at[1])
    wait_for(tok.at[low, of_right], tfrom_right.at[0])
    wait_for(tok.at[low, of_far], tf_recv.at[0])
    wait_for(tok.at[high, of_far], tf_recv.at[1])

    def stream_rows(r):
        at = rows_at(r, 32)
        inv = inverse[at, :]
        unit = stream[at, :].astype(F32) * inv
        unit_grad = tok[at, :].astype(F32) * gain[...]
        along = jnp.mean(unit * unit_grad, axis=-1, keepdims=True)
        sgrad[at, :] = (cot[at, :].astype(F32) + inv * (unit_grad - unit * along)).astype(BF)

    loop(0, tokens // 32, stream_rows)

    block = width // experts
    pairs = experts // 2
    core = lax.rem(me, 2)
    here = lax.div(me, 2)
    groups = plane // 2
    cut = plane * block

    line = lax.rem(here, groups)

    def plane_of(j):
        half = lax.div(j + 1, 2)
        return lax.rem(z + 4 + half - 2 * half * lax.rem(j, 2), 8)

    def out_rows(j):
        at = plane_of(j)
        found = rows_product(sgrad[:, rows_at(at, cut)], mixed[...]).astype(BF)
        of_plane = rows_at(at, groups)
        owp[of_plane] = found.reshape(groups, 2, block, found.shape[-1])
        copy_to(owp.at[of_plane, 1 - core], pair.at[of_plane], pair_send.at[j], pair_recv.at[j], me + 1 - 2 * core, q)

    loop(0, 8, out_rows)

    def pair_sum(j):
        at = plane_of(j)
        of_plane = rows_at(at, groups)
        wait_for(pair.at[of_plane], pair_recv.at[j])
        psum[of_plane] = (owp[of_plane, core].astype(F32) + pair[of_plane].astype(F32)).astype(BF)

        def send_sum(k):
            to = lax.rem(line + k, groups)
            copy_to(
                psum.at[at * groups + to], row_in.at[k - 1, at], row_send, row_recv.at[j], 2 * (z * groups + to) + core, q
            )

        loop(1, groups, send_sum)

    loop(0, 8, pair_sum)

    mixed_grad = product_of(sgrad[...], ow[...])
    fgrad[0:tokens, :] = mixed_grad * og[...].astype(F32)

    @pl.when(me > 0)
    def _():
        copy_to(fgrad.at[0:8], fgrad.at[tokens : tokens + 8], one_send.at[3], one_recv.at[3], me - 1, q)

    @pl.when(me == experts - 1)
    def _():
        fgrad[tokens : tokens + 8, :] = jnp.zeros((8, part_of(fgrad)), F32)

    def row_sum(j):
        at = plane_of(j)
        found = psum[at * groups + line].astype(F32)
        if groups > 1:
            wait_for(row_in.at[:, at], row_recv.at[j])
            for k in range(groups - 1):
                found = found + row_in[k, at].astype(F32)
        row_total[at] = found.astype(BF)

        @pl.when(at != z)
        def _():
            copy_to(row_total.at[at], arrived.at[z], one_send.at[4], one_recv.at[4], 2 * (at * groups + line) + core, q)

    loop(0, 8, row_sum)
    arrived[z] = row_total[z]
    og_out[...] = (mixed_grad * filtered[...]).astype(BF)
    finished[1].start()
    stream_out[...] = sgrad[:, mine]
    finished[0].start()

    @pl.when(me < experts - 1)
    def _():
        wait_for(fgrad.at[tokens : tokens + 8], one_recv.at[3])

    product_grad = (
        taps[0:1, :] * fgrad[0:tokens, :] + taps[1:2, :] * fgrad[1 : tokens + 1, :] + taps[2:3, :] * fgrad[2 : tokens + 2, :]
    )
    ig_out[...] = (product_grad * ci[...].astype(F32)).astype(BF)
    ci_out[...] = (product_grad * ig[...].astype(F32)).astype(BF)
    finished[2].start()
    finished[3].start()

    def sent_rows(t):
        @pl.when((t >= 1) & (t < 6))
        def _():
            piece = rows.at[:, rows_at(0, span), mine]
            wait_for(piece, a_send.at[t])
            wait_for(piece, right_send.at[t])
            wait_for(piece, left_send.at[t])
            wait_for(rows.at[0, rows_at(0, span), mine], fright_send.at[t])
            wait_for(rows.at[0, rows_at(0, span), mine], fleft_send.at[t])

        @pl.when(t == 0)
        def _():
            if plane > 1:
                wait_for(rows.at[:, pl.ds(0, (plane - 1) * CAP), :], a_send.at[0])

        @pl.when(t >= 6)
        def _():
            wait_for(rows.at[:, rows_at(0, span), :], a_send.at[t])

        wait_for(summand.at[:, rows_at(0, span), :], rs_send.at[t])
        wait_for(summand.at[0, rows_at(0, span), :], far_send.at[t])

    loop(0, 8, sent_rows)
    wait_for(back.at[pl.ds(0, (experts - 1) * CAP), :], one_send.at[1])
    for h in range(2):
        wait_for(tok.at[low, mine], tright_send.at[h])
        wait_for(tok.at[low, mine], tleft_send.at[h])
        wait_for(tok.at[low, mine], tf_send.at[h])

    def pair_sent(j):
        wait_for(pair.at[pl.ds(0, groups)], pair_send.at[j])

    loop(0, 8, pair_sent)
    if groups > 1:
        wait_for(psum.at[pl.ds(0, 8 * (groups - 1))], row_send)

    @pl.when(me < experts - 1)
    def _():
        wait_for(extended.at[0:8], one_send.at[0])

    @pl.when(me > 0)
    def _():
        wait_for(fgrad.at[0:8], one_send.at[3])

    wait_for(arrived.at[pl.ds(0, 7)], one_recv.at[4])
    added = arrived[0].astype(F32)
    for p in range(1, 8):
        added = added + arrived[p].astype(F32)
    ow_out[...] = added
    finished[4].start()
    for copy in finished:
        copy.wait()
    wait_for(arrived.at[pl.ds(0, 7)], one_send.at[4])


def part_of(ref):
    return ref.shape[-1]


def whole_step(choice, scale, gain, taps, stream, cot, ig, ci, og, wg, wu, wd, ow, experts):
    tokens, width = cot.shape
    part = width // 4
    slots = experts * CAP
    plane = experts // 8
    hid = wg.shape[1]
    chan = og.shape[1]
    block = width // experts
    vm = pl.BlockSpec(memory_space=pltpu.VMEM)
    hbm = pl.BlockSpec(memory_space=pltpu.HBM)
    dma = pltpu.SemaphoreType.DMA
    return pl.pallas_call(
        functools.partial(step_kernel, plane),
        name="experts",
        out_shape=(
            jax.ShapeDtypeStruct((tokens, part), BF),
            jax.ShapeDtypeStruct((tokens, chan), BF),
            jax.ShapeDtypeStruct((tokens, chan), BF),
            jax.ShapeDtypeStruct((tokens, chan), BF),
            jax.ShapeDtypeStruct((block, chan), F32),
            jax.ShapeDtypeStruct((width, hid), BF),
            jax.ShapeDtypeStruct((width, hid), BF),
            jax.ShapeDtypeStruct((hid, width), BF),
        ),
        in_specs=[vm] * 4 + [hbm] * 9,
        out_specs=(hbm,) * 8,
        scratch_shapes=[
            pltpu.VMEM((tokens, width), BF),
            pltpu.VMEM((tokens, width), BF),
            pltpu.VMEM((tokens, chan), BF),
            pltpu.VMEM((tokens, chan), BF),
            pltpu.VMEM((tokens, chan), BF),
            pltpu.VMEM((width, hid), BF),
            pltpu.VMEM((width, hid), BF),
            pltpu.VMEM((hid, width), BF),
            pltpu.VMEM((width, chan), BF),
            pltpu.VMEM((tokens, 1), F32),
            pltpu.VMEM((tokens, width), BF),
            pltpu.VMEM((slots, tokens), BF),
            pltpu.VMEM((slots, 1), F32),
            pltpu.VMEM((3, 2, plane * CAP, width), BF),
            pltpu.VMEM((5, 2, plane * CAP, part), BF),
            pltpu.VMEM((2, slots, width), BF),
            pltpu.VMEM((slots, width), BF),
            pltpu.VMEM((2, slots, part), BF),
            pltpu.VMEM((2, slots // 2, part), BF),
            pltpu.VMEM((2, slots // 2, part), BF),
            pltpu.VMEM((slots, part), BF),
            pltpu.VMEM((slots, part), BF),
            pltpu.VMEM((slots, hid), BF),
            pltpu.VMEM((slots, hid), BF),
            pltpu.VMEM((slots, hid), BF),
            pltpu.VMEM((width, hid), BF),
            pltpu.VMEM((width, hid), BF),
            pltpu.VMEM((hid, width), BF),
            pltpu.VMEM((tokens, width), BF),
            pltpu.VMEM((tokens, width), BF),
            pltpu.VMEM((tokens + 8, chan), F32),
            pltpu.VMEM((tokens, chan), F32),
            pltpu.VMEM((tokens, chan), BF),
            pltpu.VMEM((tokens + 8, chan), F32),
            pltpu.VMEM((experts // 2, 2, block, chan), BF),
            pltpu.VMEM((experts // 2, block, chan), BF),
            pltpu.VMEM((experts // 2, block, chan), BF),
            pltpu.VMEM((max(1, plane // 2 - 1), 8, block, chan), BF),
            pltpu.VMEM((8, block, chan), BF),
            pltpu.VMEM((8, block, chan), BF),
            pltpu.VMEM((width, hid), F32),
            pltpu.VMEM((width, hid), F32),
            pltpu.VMEM((hid, width), F32),
            pltpu.VMEM((tokens, part), BF),
            pltpu.VMEM((tokens, chan), BF),
            pltpu.VMEM((tokens, chan), BF),
            pltpu.VMEM((tokens, chan), BF),
            pltpu.VMEM((block, chan), F32),
            dma((9,)),
            dma((8,)),
        ]
        + [dma((8,))] * 2
        + [dma((16,))]
        + [dma((8,))] * 14
        + [dma((2,))] * 6
        + [dma((5,))] * 2
        + [dma((8,))] * 2
        + [dma, dma((8,))],
        compiler_params=pltpu.CompilerParams(
            collective_id=0, has_side_effects=True, vmem_limit_bytes=62 * 1024 * 1024
        ),
    )(choice, scale, gain, taps, stream, cot, ig, ci, og, wg, wu, wd, ow)


def finish_kernel(pieces, *refs):
    given, outs, held, wide, in_sem, out_sem = refs[:8], refs[8:16], refs[16:24], refs[24:27], refs[27], refs[28]

    def cut(k):
        rows = given[k].shape[0] // pieces
        return [pl.ds(n * rows, rows) for n in range(pieces)] if k > 4 else [pl.ds(0, given[k].shape[0])]

    order = [(k, at) for k in (5, 6, 7, 0, 1, 2, 3, 4) for at in cut(k)]
    arriving = [pltpu.make_async_copy(given[k].at[at], held[k].at[at], in_sem.at[n]) for n, (k, at) in enumerate(order)]
    leaving = [
        pltpu.make_async_copy(wide[k - 5].at[at] if k > 4 else held[k].at[at], outs[k].at[at], out_sem.at[n])
        for n, (k, at) in enumerate(order)
    ]
    for copy in arriving:
        copy.start()
    for (k, at), copy, then in zip(order, arriving, leaving):
        copy.wait()
        if k > 4:
            wide[k - 5][at] = held[k][at].astype(F32)
        then.start()
    for copy in leaving:
        copy.wait()


def finished_outputs(arrays, pieces):
    types = [F32 if k > 3 else BF for k in range(len(arrays))]
    hbm = pl.BlockSpec(memory_space=pltpu.HBM)
    count = 5 + 3 * pieces
    return pl.pallas_call(
        functools.partial(finish_kernel, pieces),
        name="finish",
        out_shape=[jax.ShapeDtypeStruct(a.shape, t) for a, t in zip(arrays, types)],
        in_specs=[hbm] * 8,
        out_specs=[hbm] * 8,
        scratch_shapes=[pltpu.VMEM(a.shape, a.dtype) for a in arrays]
        + [pltpu.VMEM(a.shape, F32) for a in arrays[5:]]
        + [pltpu.SemaphoreType.DMA((count,)), pltpu.SemaphoreType.DMA((count,))],
        compiler_params=pltpu.CompilerParams(vmem_limit_bytes=60 * 1024 * 1024),
    )(*arrays)


def shards(
    cotangent,
    stream_in,
    norm_gain,
    out_gate,
    in_gate,
    conv_input,
    conv_taps,
    out_weight,
    expert_gate,
    expert_up,
    expert_down,
    expert_choice,
    route_scale,
):
    sp_size = lax.axis_size("sp")
    arrays = whole_step(
        expert_choice.T, route_scale.T, norm_gain[None], conv_taps, stream_in, cotangent, in_gate, conv_input, out_gate,
        expert_gate[0], expert_up[0], expert_down[0], out_weight, sp_size,
    )
    *others, grad_gate, grad_up, grad_down = finished_outputs(arrays, 4)
    return (*others, grad_gate[None], grad_up[None], grad_down[None])


def solution(mesh):
    placed = (
        P("sp", None),
        P("sp", None),
        P(),
        P("sp", "tp"),
        P("sp", "tp"),
        P("sp", "tp"),
        P(None, "tp"),
        P(None, "tp"),
        P("sp", None, "tp"),
        P("sp", None, "tp"),
        P("sp", "tp", None),
        P("sp", None),
        P("sp", None),
    )
    return jax.shard_map(
        shards,
        mesh=mesh,
        in_specs=placed,
        out_specs=(
            P("sp", "tp"),
            P("sp", "tp"),
            P("sp", "tp"),
            P("sp", "tp"),
            P("sp", "tp"),
            P("sp", None, "tp"),
            P("sp", None, "tp"),
            P("sp", "tp", None),
        ),
        check_vma=False,
    )
```

```python
import functools

import jax
import jax.numpy as jnp
from jax import lax
from jax.experimental import pallas as pl
from jax.experimental.pallas import tpu as pltpu
from jax.sharding import PartitionSpec as P

norm_eps = 1e-06
MESH = pl.DeviceIdType.MESH
CAP = 16
BF = jnp.bfloat16
F32 = jnp.float32


def rows_product(left, right):
    return lax.dot_general(left, right, (((0,), (0,)), ((), ())), preferred_element_type=F32)


def cols_product(left, right):
    return lax.dot_general(left, right, (((1,), (1,)), ((), ())), preferred_element_type=F32)


def product_of(left, right):
    return jnp.dot(left, right, preferred_element_type=F32)


def loop(low, high, body):
    def step(i, carry):
        body(i)
        return carry

    lax.fori_loop(low, high, step, 0)


def offset_of(t):
    half = lax.div(t + 1, 2)
    odd = lax.rem(t, 2)
    spread = odd * (1 + half) + (1 - odd) * (7 - half)
    return spread + 7 * lax.div(t + 7, 8) - 7 + 3 * lax.div(t, 6) - 7 * lax.div(t, 7)


def rows_at(index, count):
    return pl.ds(pl.multiple_of(index * count, count), count)


def step_kernel(
    plane, choice, scale, gain, taps, stream_hbm, cot_hbm, ig_hbm, ci_hbm, og_hbm, wg_hbm, wu_hbm, wd_hbm, ow_hbm,
    *refs,
):
    outs, refs = refs[:8], refs[8:]
    (
        stream, cot, ig, ci, og, wg, wu, wd, ow, inverse, normed, pick, weight, send_all, send_part, rows, partial, summand, far_in, far_sum, total, back,
        hidden, ggrad, ugrad, gate_out, up_out, down_out, tok, sgrad, extended, filtered, mixed, fgrad,
        owp, pair, psum, row_in, row_total, arrived, gate_sum, up_sum, down_sum,
        stream_out, og_out, ig_out, ci_out, ow_out,
        in_sem, out_sem,
        a_send, a_recv, half_recv, right_send, left_send, from_left, from_right,
        fright_send, fleft_send, ffrom_left, ffrom_right,
        rs_send, far_send, of_left_recv, of_right_recv, far_left_recv, far_right_recv, tright_send, tleft_send, tfrom_left, tfrom_right, tf_send, tf_recv, one_send, one_recv, pair_send, pair_recv, row_send, row_recv,
    ) = refs
    me = lax.axis_index("sp")
    q = lax.axis_index("tp")
    right = lax.rem(q + 1, 4)
    left = lax.rem(q + 3, 4)
    z = lax.div(me, plane)
    place = lax.rem(me, plane)
    experts = 8 * plane
    span = plane * CAP
    tokens, width = cot.shape
    part = width // 4
    mine = rows_at(q, part)
    of_left = rows_at(left, part)
    of_right = rows_at(right, part)
    of_far = rows_at(lax.rem(q + 2, 4), part)
    my_slots = rows_at(me, CAP)

    def copy_to(src, dst, send, recv, sp, tp):
        pltpu.make_async_remote_copy(src, dst, send, recv, device_id=(sp, tp), device_id_type=MESH).start()

    def wait_for(ref, sem):
        pltpu.make_async_copy(ref, ref, sem).wait()

    def source_at(t):
        return lax.rem(z + 8 - offset_of(t), 8)

    def next_place(k):
        return lax.rem(place + k, plane)

    given = (stream_hbm, cot_hbm, ig_hbm, ci_hbm, og_hbm, wg_hbm, wu_hbm, wd_hbm, ow_hbm)
    held = (stream, cot, ig, ci, og, wg, wu, wd, ow)
    copies = [pltpu.make_async_copy(a, b, in_sem.at[n]) for n, (a, b) in enumerate(zip(given, held))]
    for copy in copies:
        copy.start()

    barrier = pltpu.get_barrier_semaphore()

    def greet(k):
        pl.semaphore_signal(barrier, inc=1, device_id=(lax.rem(me + k, experts), q), device_id_type=MESH)

    loop(1, experts, greet)

    def greet_row(k):
        pl.semaphore_signal(barrier, inc=1, device_id=(me, lax.rem(q + k, 4)), device_id_type=MESH)

    loop(1, 4, greet_row)

    first, second = choice[0:1, :], choice[1:2, :]
    ids = lax.broadcasted_iota(jnp.int32, (experts, tokens), 0)
    is_first, is_second = ids == first, ids == second
    named = jnp.where(is_first | is_second, 1.0, 0.0).astype(BF)
    before = jnp.where(
        lax.broadcasted_iota(jnp.int32, (tokens, tokens), 0) < lax.broadcasted_iota(jnp.int32, (tokens, tokens), 1), 1.0, 0.0
    ).astype(BF)
    earlier = product_of(named, before)
    slot_first = first * CAP + jnp.sum(jnp.where(is_first, earlier, 0.0), axis=0, keepdims=True).astype(jnp.int32)
    slot_second = second * CAP + jnp.sum(jnp.where(is_second, earlier, 0.0), axis=0, keepdims=True).astype(jnp.int32)

    def pick_rows(p):
        slots = lax.broadcasted_iota(jnp.int32, (span, tokens), 0) + p * span
        at_first, at_second = slots == slot_first, slots == slot_second
        pick[rows_at(p, span), :] = jnp.where(at_first | at_second, 1.0, 0.0).astype(BF)
        weight[rows_at(p, span), :] = jnp.sum(
            jnp.where(at_first, scale[0:1, :], 0.0) + jnp.where(at_second, scale[1:2, :], 0.0), axis=1, keepdims=True
        )

    loop(0, 8, pick_rows)

    copies[0].wait()

    def norm_rows(r):
        at = rows_at(r, 32)
        x = stream[at, :].astype(F32)
        inv = lax.rsqrt(jnp.mean(x * x, axis=-1, keepdims=True) + norm_eps)
        inverse[at, :] = inv
        normed[at, :] = ((x * inv) * gain[...]).astype(BF)

    loop(0, tokens // 32, norm_rows)

    copies[1].wait()

    def fill_quarter(t):
        at = rows_at(lax.rem(z + offset_of(t), 8), span)
        chosen = pick[at, :]
        send_part[t - 1, 0] = product_of(chosen, normed[:, mine]).astype(BF)
        send_part[t - 1, 1] = (product_of(chosen, cot[:, mine]) * weight[at, :]).astype(BF)

    loop(1, 6, fill_quarter)

    copies[2].wait()
    copies[3].wait()
    extended[8 : tokens + 8, :] = ig[...].astype(F32) * ci[...].astype(F32)

    @pl.when(me == 0)
    def _():
        extended[0:8, :] = jnp.zeros((8, part_of(extended)), F32)

    pl.semaphore_wait(barrier, experts + 2)

    @pl.when(me < experts - 1)
    def _():
        copy_to(extended.at[tokens : tokens + 8], extended.at[0:8], one_send.at[0], one_recv.at[0], me + 1, q)

    side = plane // 2

    def send_quarter(t):
        target = lax.rem(z + offset_of(t), 8)

        def one(k):
            turn = lax.div(k, side)
            block = lax.rem(lax.div(place, side) + turn, 2)
            to = block * side + lax.rem(place + k, side)
            copy_to(
                send_part.at[t - 1, :, rows_at(to, CAP), :], rows.at[:, my_slots, mine],
                a_send.at[t], half_recv.at[2 * t + turn], target * plane + to, q,
            )

        loop(0, plane, one)

    loop(1, 6, send_quarter)

    def turn_of(i):
        return i + 5 * lax.div(i + 1, 2)

    def fill_whole(i):
        at = rows_at(lax.rem(z + offset_of(turn_of(i)), 8), span)
        chosen = pick[at, :]
        send_all[i, 0] = product_of(chosen, normed[...]).astype(BF)
        send_all[i, 1] = (product_of(chosen, cot[...]) * weight[at, :]).astype(BF)

    loop(0, 3, fill_whole)
    own = rows_at(place, CAP)
    rows[0, my_slots, :] = send_all[0, 0, own, :]
    rows[1, my_slots, :] = send_all[0, 1, own, :]

    def send_whole(i):
        t = turn_of(i)
        target = lax.rem(z + offset_of(t), 8)

        def one(k):
            to = next_place(k)

            @pl.when(target * plane + to != me)
            def _():
                copy_to(
                    send_all.at[i, :, rows_at(to, CAP), :], rows.at[:, my_slots, :],
                    a_send.at[t], a_recv.at[t], target * plane + to, q,
                )

        loop(0, plane, one)


    send_whole(0)

    @pl.when(me > 0)
    def _():
        wait_for(extended.at[0:8], one_recv.at[0])

    copies[4].wait()
    now = (
        taps[0:1, :] * extended[8 : tokens + 8, :]
        + taps[1:2, :] * extended[7 : tokens + 7, :]
        + taps[2:3, :] * extended[6 : tokens + 6, :]
    )
    filtered[...] = now
    mixed[...] = (og[...].astype(F32) * now).astype(BF)
    chunk = min(256, width)

    def clear(m):
        cols = rows_at(m, chunk)
        gate_sum[cols, :] = jnp.zeros((chunk, part_of(gate_sum)), F32)
        up_sum[cols, :] = jnp.zeros((chunk, part_of(up_sum)), F32)
        down_sum[:, cols] = jnp.zeros((down_sum.shape[0], chunk), F32)

    loop(0, width // chunk, clear)
    for copy in copies[5:]:
        copy.wait()

    def add_grads(at):
        def one(m):
            cols = rows_at(m, chunk)
            here = rows[0, at, cols]
            gate_sum[cols, :] += rows_product(here, ggrad[at, :])
            up_sum[cols, :] += rows_product(here, ugrad[at, :])
            down_sum[:, cols] += rows_product(hidden[at, :], rows[1, at, cols])

        loop(0, width // chunk, one)

    def halves_at(t):
        source = source_at(t)
        return rows_at(2 * source, span // 2), rows_at(2 * source + 1, span // 2), source

    def pass_sum(t):
        upper, lower, source = halves_at(t)
        held_at = rows_at(source, span // 2)
        wait_for(far_in.at[0, held_at, :], far_left_recv.at[t])
        far_sum[0, held_at, :] = (partial[upper, of_right].astype(F32) + far_in[0, held_at, :].astype(F32)).astype(BF)
        copy_to(far_sum.at[0, held_at, :], summand.at[0, upper, :], rs_send.at[t], of_left_recv.at[t], me, right)
        wait_for(far_in.at[1, held_at, :], far_right_recv.at[t])
        far_sum[1, held_at, :] = (partial[lower, of_left].astype(F32) + far_in[1, held_at, :].astype(F32)).astype(BF)
        copy_to(far_sum.at[1, held_at, :], summand.at[1, lower, :], rs_send.at[t], of_right_recv.at[t], me, left)

    def step(i):
        @pl.when((i >= 1) & (i < 6))
        def _():
            for turn in range(2):
                block = lax.rem(lax.div(place, side) + turn, 2)
                piece = rows.at[:, rows_at(2 * source_at(i) + block, span // 2), mine]
                wait_for(piece, half_recv.at[2 * i + turn])
                copy_to(piece, piece, right_send.at[i], from_left.at[i], me, right)
                copy_to(piece, piece, left_send.at[i], from_right.at[i], me, left)

        @pl.when(i == 3)
        def _():
            send_whole(1)
            send_whole(2)

        @pl.when((i >= 2) & (i < 7))
        def _():
            t = i - 1
            at = rows_at(source_at(t), span)
            wait_for(rows.at[:, at, of_left], from_left.at[t])
            half = rows.at[0, at, of_left]
            copy_to(half, half, fright_send.at[t], ffrom_left.at[t], me, right)
            wait_for(rows.at[:, at, of_right], from_right.at[t])
            half = rows.at[1, at, of_right]
            copy_to(half, half, fleft_send.at[t], ffrom_right.at[t], me, left)

        @pl.when((i >= 3) & (i < 8))
        def _():
            pass_sum(i - 3)

        @pl.when((i >= 2) & (i < 10))
        def _():
            t = i - 2
            at = rows_at(source_at(t), span)

            @pl.when((t >= 1) & (t < 6))
            def _():
                wait_for(rows.at[0, at, of_far], ffrom_left.at[t])
                wait_for(rows.at[1, at, of_far], ffrom_right.at[t])

            @pl.when(t == 0)
            def _():
                if plane > 1:
                    wait_for(rows.at[:, pl.ds(0, (plane - 1) * CAP), :], a_recv.at[0])

            @pl.when(t >= 6)
            def _():
                wait_for(rows.at[:, at, :], a_recv.at[t])

            here = rows[0, at, :]
            gate_pre = product_of(here, wg[...])
            up_pre = product_of(here, wu[...])
            hidden_grad = cols_product(rows[1, at, :], wd[...])
            sigmoid_gate = jax.nn.sigmoid(gate_pre)
            silu_gate = gate_pre * sigmoid_gate
            hidden[at, :] = (silu_gate * up_pre).astype(BF)
            gate_grad = (hidden_grad * up_pre * sigmoid_gate * (1.0 + gate_pre * (1.0 - sigmoid_gate))).astype(BF)
            up_grad = (hidden_grad * silu_gate).astype(BF)
            ggrad[at, :] = gate_grad
            ugrad[at, :] = up_grad
            partial[at, :] = (cols_product(gate_grad, wg[...]) + cols_product(up_grad, wu[...])).astype(BF)

            upper, lower, source = halves_at(t)
            held_at = rows_at(source, span // 2)
            copy_to(partial.at[upper, of_far], far_in.at[0, held_at, :], far_send.at[t], far_left_recv.at[t], me, right)
            copy_to(partial.at[lower, of_far], far_in.at[1, held_at, :], far_send.at[t], far_right_recv.at[t], me, left)
            copy_to(partial.at[lower, of_right], summand.at[0, lower, :], rs_send.at[t], of_left_recv.at[t], me, right)
            copy_to(partial.at[upper, of_left], summand.at[1, upper, :], rs_send.at[t], of_right_recv.at[t], me, left)

            @pl.when(t < 5)
            def _():
                add_grads(at)

        @pl.when((i >= 8) & (i < 11))
        def _():
            pass_sum(i - 3)

        @pl.when(i >= 4)
        def _():
            t = i - 4
            source = source_at(t)
            at = rows_at(source, span)
            wait_for(summand.at[0, at, :], of_left_recv.at[t])
            wait_for(summand.at[1, at, :], of_right_recv.at[t])
            added = partial[at, mine].astype(F32) + summand[0, at, :].astype(F32) + summand[1, at, :].astype(F32)
            total[at, :] = added.astype(BF)

            def one(k):
                to = source * plane + next_place(k)

                @pl.when(to != me)
                def _():
                    copy_to(total.at[rows_at(to, CAP), :], back.at[my_slots, :], one_send.at[1], one_recv.at[1], to, q)

            loop(0, plane, one)

    loop(1, 12, step)
    back[my_slots, :] = total[my_slots, :]

    def late_grads(t):
        add_grads(rows_at(source_at(t), span))

    loop(5, 7, late_grads)

    wait_for(back.at[pl.ds(0, (experts - 1) * CAP), :], one_recv.at[1])
    tok[:, mine] = rows_product(pick[...], back[...]).astype(BF)
    half = tokens // 2
    low, high = pl.ds(0, half), pl.ds(half, half)
    for h, at in ((0, low), (1, high)):
        copy_to(tok.at[at, mine], tok.at[at, mine], tright_send.at[h], tfrom_left.at[h], me, right)
    for h, at in ((1, high), (0, low)):
        copy_to(tok.at[at, mine], tok.at[at, mine], tleft_send.at[h], tfrom_right.at[h], me, left)
    loop(7, 8, late_grads)
    wait_for(tok.at[low, of_left], tfrom_left.at[0])
    copy_to(tok.at[low, of_left], tok.at[low, of_left], tf_send.at[0], tf_recv.at[0], me, right)
    wait_for(tok.at[high, of_right], tfrom_right.at[1])
    copy_to(tok.at[high, of_right], tok.at[high, of_right], tf_send.at[1], tf_recv.at[1], me, left)
    def narrow(m):
        cols = rows_at(m, chunk)
        gate_out[cols, :] = gate_sum[cols, :].astype(BF)
        up_out[cols, :] = up_sum[cols, :].astype(BF)
        down_out[:, cols] = down_sum[:, cols].astype(BF)

    loop(0, width // chunk, narrow)
    ready = (stream_out, og_out, ig_out, ci_out, ow_out, gate_out, up_out, down_out)
    finished = [pltpu.make_async_copy(a, b, out_sem.at[n]) for n, (a, b) in enumerate(zip(ready, outs))]
    for copy in finished[5:]:
        copy.start()

    wait_for(tok.at[high, of_left], tfrom_left.at[1])
    wait_for(tok.at[low, of_right], tfrom_right.at[0])
    wait_for(tok.at[low, of_far], tf_recv.at[0])
    wait_for(tok.at[high, of_far], tf_recv.at[1])

    def stream_rows(r):
        at = rows_at(r, 32)
        inv = inverse[at, :]
        unit = stream[at, :].astype(F32) * inv
        unit_grad = tok[at, :].astype(F32) * gain[...]
        along = jnp.mean(unit * unit_grad, axis=-1, keepdims=True)
        sgrad[at, :] = (cot[at, :].astype(F32) + inv * (unit_grad - unit * along)).astype(BF)

    loop(0, tokens // 32, stream_rows)

    block = width // experts
    pairs = experts // 2
    core = lax.rem(me, 2)
    here = lax.div(me, 2)
    groups = plane // 2
    cut = plane * block

    line = lax.rem(here, groups)

    def plane_of(j):
        half = lax.div(j + 1, 2)
        return lax.rem(z + 4 + half - 2 * half * lax.rem(j, 2), 8)

    def out_rows(j):
        at = plane_of(j)
        found = rows_product(sgrad[:, rows_at(at, cut)], mixed[...]).astype(BF)
        of_plane = rows_at(at, groups)
        owp[of_plane] = found.reshape(groups, 2, block, found.shape[-1])
        copy_to(owp.at[of_plane, 1 - core], pair.at[of_plane], pair_send.at[j], pair_recv.at[j], me + 1 - 2 * core, q)

    loop(0, 8, out_rows)

    def pair_sum(j):
        at = plane_of(j)
        of_plane = rows_at(at, groups)
        wait_for(pair.at[of_plane], pair_recv.at[j])
        psum[of_plane] = (owp[of_plane, core].astype(F32) + pair[of_plane].astype(F32)).astype(BF)

        def send_sum(k):
            to = lax.rem(line + k, groups)
            copy_to(
                psum.at[at * groups + to], row_in.at[k - 1, at], row_send, row_recv.at[j], 2 * (z * groups + to) + core, q
            )

        loop(1, groups, send_sum)

    loop(0, 8, pair_sum)

    mixed_grad = product_of(sgrad[...], ow[...])
    fgrad[0:tokens, :] = mixed_grad * og[...].astype(F32)

    @pl.when(me > 0)
    def _():
        copy_to(fgrad.at[0:8], fgrad.at[tokens : tokens + 8], one_send.at[3], one_recv.at[3], me - 1, q)

    @pl.when(me == experts - 1)
    def _():
        fgrad[tokens : tokens + 8, :] = jnp.zeros((8, part_of(fgrad)), F32)

    def row_sum(j):
        at = plane_of(j)
        found = psum[at * groups + line].astype(F32)
        if groups > 1:
            wait_for(row_in.at[:, at], row_recv.at[j])
            for k in range(groups - 1):
                found = found + row_in[k, at].astype(F32)
        row_total[at] = found.astype(BF)

        @pl.when(at != z)
        def _():
            copy_to(row_total.at[at], arrived.at[z], one_send.at[4], one_recv.at[4], 2 * (at * groups + line) + core, q)

    loop(0, 8, row_sum)
    arrived[z] = row_total[z]
    og_out[...] = (mixed_grad * filtered[...]).astype(BF)
    finished[1].start()
    stream_out[...] = sgrad[:, mine]
    finished[0].start()

    @pl.when(me < experts - 1)
    def _():
        wait_for(fgrad.at[tokens : tokens + 8], one_recv.at[3])

    product_grad = (
        taps[0:1, :] * fgrad[0:tokens, :] + taps[1:2, :] * fgrad[1 : tokens + 1, :] + taps[2:3, :] * fgrad[2 : tokens + 2, :]
    )
    ig_out[...] = (product_grad * ci[...].astype(F32)).astype(BF)
    ci_out[...] = (product_grad * ig[...].astype(F32)).astype(BF)
    finished[2].start()
    finished[3].start()

    def sent_rows(t):
        @pl.when((t >= 1) & (t < 6))
        def _():
            piece = rows.at[:, rows_at(0, span), mine]
            wait_for(piece, a_send.at[t])
            wait_for(piece, right_send.at[t])
            wait_for(piece, left_send.at[t])
            wait_for(rows.at[0, rows_at(0, span), mine], fright_send.at[t])
            wait_for(rows.at[0, rows_at(0, span), mine], fleft_send.at[t])

        @pl.when(t == 0)
        def _():
            if plane > 1:
                wait_for(rows.at[:, pl.ds(0, (plane - 1) * CAP), :], a_send.at[0])

        @pl.when(t >= 6)
        def _():
            wait_for(rows.at[:, rows_at(0, span), :], a_send.at[t])

        wait_for(summand.at[:, rows_at(0, span), :], rs_send.at[t])
        wait_for(summand.at[0, rows_at(0, span), :], far_send.at[t])

    loop(0, 8, sent_rows)
    wait_for(back.at[pl.ds(0, (experts - 1) * CAP), :], one_send.at[1])
    for h in range(2):
        wait_for(tok.at[low, mine], tright_send.at[h])
        wait_for(tok.at[low, mine], tleft_send.at[h])
        wait_for(tok.at[low, mine], tf_send.at[h])

    def pair_sent(j):
        wait_for(pair.at[pl.ds(0, groups)], pair_send.at[j])

    loop(0, 8, pair_sent)
    if groups > 1:
        wait_for(psum.at[pl.ds(0, 8 * (groups - 1))], row_send)

    @pl.when(me < experts - 1)
    def _():
        wait_for(extended.at[0:8], one_send.at[0])

    @pl.when(me > 0)
    def _():
        wait_for(fgrad.at[0:8], one_send.at[3])

    wait_for(arrived.at[pl.ds(0, 7)], one_recv.at[4])
    added = arrived[0].astype(F32)
    for p in range(1, 8):
        added = added + arrived[p].astype(F32)
    ow_out[...] = added
    finished[4].start()
    for copy in finished:
        copy.wait()
    wait_for(arrived.at[pl.ds(0, 7)], one_send.at[4])


def part_of(ref):
    return ref.shape[-1]


def whole_step(choice, scale, gain, taps, stream, cot, ig, ci, og, wg, wu, wd, ow, experts):
    tokens, width = cot.shape
    part = width // 4
    slots = experts * CAP
    plane = experts // 8
    hid = wg.shape[1]
    chan = og.shape[1]
    block = width // experts
    vm = pl.BlockSpec(memory_space=pltpu.VMEM)
    hbm = pl.BlockSpec(memory_space=pltpu.HBM)
    dma = pltpu.SemaphoreType.DMA
    return pl.pallas_call(
        functools.partial(step_kernel, plane),
        name="experts",
        out_shape=(
            jax.ShapeDtypeStruct((tokens, part), BF),
            jax.ShapeDtypeStruct((tokens, chan), BF),
            jax.ShapeDtypeStruct((tokens, chan), BF),
            jax.ShapeDtypeStruct((tokens, chan), BF),
            jax.ShapeDtypeStruct((block, chan), F32),
            jax.ShapeDtypeStruct((width, hid), BF),
            jax.ShapeDtypeStruct((width, hid), BF),
            jax.ShapeDtypeStruct((hid, width), BF),
        ),
        in_specs=[vm] * 4 + [hbm] * 9,
        out_specs=(hbm,) * 8,
        scratch_shapes=[
            pltpu.VMEM((tokens, width), BF),
            pltpu.VMEM((tokens, width), BF),
            pltpu.VMEM((tokens, chan), BF),
            pltpu.VMEM((tokens, chan), BF),
            pltpu.VMEM((tokens, chan), BF),
            pltpu.VMEM((width, hid), BF),
            pltpu.VMEM((width, hid), BF),
            pltpu.VMEM((hid, width), BF),
            pltpu.VMEM((width, chan), BF),
            pltpu.VMEM((tokens, 1), F32),
            pltpu.VMEM((tokens, width), BF),
            pltpu.VMEM((slots, tokens), BF),
            pltpu.VMEM((slots, 1), F32),
            pltpu.VMEM((3, 2, plane * CAP, width), BF),
            pltpu.VMEM((5, 2, plane * CAP, part), BF),
            pltpu.VMEM((2, slots, width), BF),
            pltpu.VMEM((slots, width), BF),
            pltpu.VMEM((2, slots, part), BF),
            pltpu.VMEM((2, slots // 2, part), BF),
            pltpu.VMEM((2, slots // 2, part), BF),
            pltpu.VMEM((slots, part), BF),
            pltpu.VMEM((slots, part), BF),
            pltpu.VMEM((slots, hid), BF),
            pltpu.VMEM((slots, hid), BF),
            pltpu.VMEM((slots, hid), BF),
            pltpu.VMEM((width, hid), BF),
            pltpu.VMEM((width, hid), BF),
            pltpu.VMEM((hid, width), BF),
            pltpu.VMEM((tokens, width), BF),
            pltpu.VMEM((tokens, width), BF),
            pltpu.VMEM((tokens + 8, chan), F32),
            pltpu.VMEM((tokens, chan), F32),
            pltpu.VMEM((tokens, chan), BF),
            pltpu.VMEM((tokens + 8, chan), F32),
            pltpu.VMEM((experts // 2, 2, block, chan), BF),
            pltpu.VMEM((experts // 2, block, chan), BF),
            pltpu.VMEM((experts // 2, block, chan), BF),
            pltpu.VMEM((max(1, plane // 2 - 1), 8, block, chan), BF),
            pltpu.VMEM((8, block, chan), BF),
            pltpu.VMEM((8, block, chan), BF),
            pltpu.VMEM((width, hid), F32),
            pltpu.VMEM((width, hid), F32),
            pltpu.VMEM((hid, width), F32),
            pltpu.VMEM((tokens, part), BF),
            pltpu.VMEM((tokens, chan), BF),
            pltpu.VMEM((tokens, chan), BF),
            pltpu.VMEM((tokens, chan), BF),
            pltpu.VMEM((block, chan), F32),
            dma((9,)),
            dma((8,)),
        ]
        + [dma((8,))] * 2
        + [dma((16,))]
        + [dma((8,))] * 14
        + [dma((2,))] * 6
        + [dma((5,))] * 2
        + [dma((8,))] * 2
        + [dma, dma((8,))],
        compiler_params=pltpu.CompilerParams(
            collective_id=0, has_side_effects=True, vmem_limit_bytes=62 * 1024 * 1024
        ),
    )(choice, scale, gain, taps, stream, cot, ig, ci, og, wg, wu, wd, ow)


def finish_kernel(pieces, *refs):
    given, outs, held, wide, in_sem, out_sem = refs[:8], refs[8:16], refs[16:24], refs[24:27], refs[27], refs[28]

    def cut(k):
        rows = given[k].shape[0] // pieces
        return [pl.ds(n * rows, rows) for n in range(pieces)] if k > 4 else [pl.ds(0, given[k].shape[0])]

    order = [(k, at) for k in (5, 6, 7, 0, 1, 2, 3, 4) for at in cut(k)]
    arriving = [pltpu.make_async_copy(given[k].at[at], held[k].at[at], in_sem.at[n]) for n, (k, at) in enumerate(order)]
    leaving = [
        pltpu.make_async_copy(wide[k - 5].at[at] if k > 4 else held[k].at[at], outs[k].at[at], out_sem.at[n])
        for n, (k, at) in enumerate(order)
    ]
    for copy in arriving:
        copy.start()
    for (k, at), copy, then in zip(order, arriving, leaving):
        copy.wait()
        if k > 4:
            wide[k - 5][at] = held[k][at].astype(F32)
        then.start()
    for copy in leaving:
        copy.wait()


def finished_outputs(arrays, pieces):
    types = [F32 if k > 3 else BF for k in range(len(arrays))]
    hbm = pl.BlockSpec(memory_space=pltpu.HBM)
    count = 5 + 3 * pieces
    return pl.pallas_call(
        functools.partial(finish_kernel, pieces),
        name="finish",
        out_shape=[jax.ShapeDtypeStruct(a.shape, t) for a, t in zip(arrays, types)],
        in_specs=[hbm] * 8,
        out_specs=[hbm] * 8,
        scratch_shapes=[pltpu.VMEM(a.shape, a.dtype) for a in arrays]
        + [pltpu.VMEM(a.shape, F32) for a in arrays[5:]]
        + [pltpu.SemaphoreType.DMA((count,)), pltpu.SemaphoreType.DMA((count,))],
        compiler_params=pltpu.CompilerParams(vmem_limit_bytes=60 * 1024 * 1024),
    )(*arrays)


def shards(
    cotangent,
    stream_in,
    norm_gain,
    out_gate,
    in_gate,
    conv_input,
    conv_taps,
    out_weight,
    expert_gate,
    expert_up,
    expert_down,
    expert_choice,
    route_scale,
):
    sp_size = lax.axis_size("sp")
    arrays = whole_step(
        expert_choice.T, route_scale.T, norm_gain[None], conv_taps, stream_in, cotangent, in_gate, conv_input, out_gate,
        expert_gate[0], expert_up[0], expert_down[0], out_weight, sp_size,
    )
    *others, grad_gate, grad_up, grad_down = finished_outputs(arrays, 4)
    return (*others, grad_gate[None], grad_up[None], grad_down[None])


def solution(mesh):
    placed = (
        P("sp", None),
        P("sp", None),
        P(),
        P("sp", "tp"),
        P("sp", "tp"),
        P("sp", "tp"),
        P(None, "tp"),
        P(None, "tp"),
        P("sp", None, "tp"),
        P("sp", None, "tp"),
        P("sp", "tp", None),
        P("sp", None),
        P("sp", None),
    )
    return jax.shard_map(
        shards,
        mesh=mesh,
        in_specs=placed,
        out_specs=(
            P("sp", "tp"),
            P("sp", "tp"),
            P("sp", "tp"),
            P("sp", "tp"),
            P("sp", "tp"),
            P("sp", None, "tp"),
            P("sp", None, "tp"),
            P("sp", "tp", None),
        ),
        check_vma=False,
    )
```

```python
import functools

import jax
import jax.numpy as jnp
from jax import lax
from jax.experimental import pallas as pl
from jax.experimental.pallas import tpu as pltpu
from jax.sharding import PartitionSpec as P

norm_eps = 1e-06
MESH = pl.DeviceIdType.MESH
CAP = 16
BF = jnp.bfloat16
F32 = jnp.float32


def rows_product(left, right):
    return lax.dot_general(left, right, (((0,), (0,)), ((), ())), preferred_element_type=F32)


def cols_product(left, right):
    return lax.dot_general(left, right, (((1,), (1,)), ((), ())), preferred_element_type=F32)


def product_of(left, right):
    return jnp.dot(left, right, preferred_element_type=F32)


def loop(low, high, body):
    def step(i, carry):
        body(i)
        return carry

    lax.fori_loop(low, high, step, 0)


def offset_of(t):
    half = lax.div(t + 1, 2)
    odd = lax.rem(t, 2)
    spread = odd * (1 + half) + (1 - odd) * (7 - half)
    return spread + 7 * lax.div(t + 7, 8) - 7 + 3 * lax.div(t, 6) - 7 * lax.div(t, 7)


def rows_at(index, count):
    return pl.ds(pl.multiple_of(index * count, count), count)


def step_kernel(
    plane, choice, scale, gain, taps, stream_hbm, cot_hbm, ig_hbm, ci_hbm, og_hbm, wg_hbm, wu_hbm, wd_hbm, ow_hbm,
    *refs,
):
    outs, refs = refs[:8], refs[8:]
    (
        stream, cot, ig, ci, og, wg, wu, wd, ow, inverse, normed, pick, weight, send_all, send_part, rows, partial, summand, far_in, far_sum, total, back,
        hidden, ggrad, ugrad, gate_out, up_out, down_out, tok, sgrad, extended, filtered, mixed, fgrad,
        owp, pair, psum, row_in, row_total, arrived, gate_sum, up_sum, down_sum,
        stream_out, og_out, ig_out, ci_out, ow_out,
        in_sem, out_sem,
        a_send, a_recv, half_recv, right_send, left_send, from_left, from_right,
        fright_send, fleft_send, ffrom_left, ffrom_right,
        rs_send, far_send, of_left_recv, of_right_recv, far_left_recv, far_right_recv, tright_send, tleft_send, tfrom_left, tfrom_right, tf_send, tf_recv, one_send, one_recv, pair_send, pair_recv, row_send, row_recv,
    ) = refs
    me = lax.axis_index("sp")
    q = lax.axis_index("tp")
    right = lax.rem(q + 1, 4)
    left = lax.rem(q + 3, 4)
    z = lax.div(me, plane)
    place = lax.rem(me, plane)
    experts = 8 * plane
    span = plane * CAP
    tokens, width = cot.shape
    part = width // 4
    mine = rows_at(q, part)
    of_left = rows_at(left, part)
    of_right = rows_at(right, part)
    of_far = rows_at(lax.rem(q + 2, 4), part)
    my_slots = rows_at(me, CAP)

    def copy_to(src, dst, send, recv, sp, tp):
        pltpu.make_async_remote_copy(src, dst, send, recv, device_id=(sp, tp), device_id_type=MESH).start()

    def wait_for(ref, sem):
        pltpu.make_async_copy(ref, ref, sem).wait()

    def source_at(t):
        return lax.rem(z + 8 - offset_of(t), 8)

    def next_place(k):
        return lax.rem(place + k, plane)

    given = (stream_hbm, cot_hbm, ig_hbm, ci_hbm, og_hbm, wg_hbm, wu_hbm, wd_hbm, ow_hbm)
    held = (stream, cot, ig, ci, og, wg, wu, wd, ow)
    copies = [pltpu.make_async_copy(a, b, in_sem.at[n]) for n, (a, b) in enumerate(zip(given, held))]
    for copy in copies:
        copy.start()

    barrier = pltpu.get_barrier_semaphore()

    def greet(k):
        pl.semaphore_signal(barrier, inc=1, device_id=(lax.rem(me + k, experts), q), device_id_type=MESH)

    loop(1, experts, greet)

    def greet_row(k):
        pl.semaphore_signal(barrier, inc=1, device_id=(me, lax.rem(q + k, 4)), device_id_type=MESH)

    loop(1, 4, greet_row)

    first, second = choice[0:1, :], choice[1:2, :]
    ids = lax.broadcasted_iota(jnp.int32, (experts, tokens), 0)
    is_first, is_second = ids == first, ids == second
    named = jnp.where(is_first | is_second, 1.0, 0.0).astype(BF)
    before = jnp.where(
        lax.broadcasted_iota(jnp.int32, (tokens, tokens), 0) < lax.broadcasted_iota(jnp.int32, (tokens, tokens), 1), 1.0, 0.0
    ).astype(BF)
    earlier = product_of(named, before)
    slot_first = first * CAP + jnp.sum(jnp.where(is_first, earlier, 0.0), axis=0, keepdims=True).astype(jnp.int32)
    slot_second = second * CAP + jnp.sum(jnp.where(is_second, earlier, 0.0), axis=0, keepdims=True).astype(jnp.int32)

    def pick_rows(p):
        slots = lax.broadcasted_iota(jnp.int32, (span, tokens), 0) + p * span
        at_first, at_second = slots == slot_first, slots == slot_second
        pick[rows_at(p, span), :] = jnp.where(at_first | at_second, 1.0, 0.0).astype(BF)
        weight[rows_at(p, span), :] = jnp.sum(
            jnp.where(at_first, scale[0:1, :], 0.0) + jnp.where(at_second, scale[1:2, :], 0.0), axis=1, keepdims=True
        )

    loop(0, 8, pick_rows)

    copies[0].wait()

    def norm_rows(r):
        at = rows_at(r, 32)
        x = stream[at, :].astype(F32)
        inv = lax.rsqrt(jnp.mean(x * x, axis=-1, keepdims=True) + norm_eps)
        inverse[at, :] = inv
        normed[at, :] = ((x * inv) * gain[...]).astype(BF)

    loop(0, tokens // 32, norm_rows)

    copies[1].wait()

    def fill_quarter(t):
        at = rows_at(lax.rem(z + offset_of(t), 8), span)
        chosen = pick[at, :]
        send_part[t - 1, 0] = product_of(chosen, normed[:, mine]).astype(BF)
        send_part[t - 1, 1] = (product_of(chosen, cot[:, mine]) * weight[at, :]).astype(BF)

    loop(1, 6, fill_quarter)

    copies[2].wait()
    copies[3].wait()
    extended[8 : tokens + 8, :] = ig[...].astype(F32) * ci[...].astype(F32)

    @pl.when(me == 0)
    def _():
        extended[0:8, :] = jnp.zeros((8, part_of(extended)), F32)

    pl.semaphore_wait(barrier, experts + 2)

    @pl.when(me < experts - 1)
    def _():
        copy_to(extended.at[tokens : tokens + 8], extended.at[0:8], one_send.at[0], one_recv.at[0], me + 1, q)

    side = plane // 2

    def send_quarter(t):
        target = lax.rem(z + offset_of(t), 8)

        def one(k):
            turn = lax.div(k, side)
            block = lax.rem(lax.div(place, side) + turn, 2)
            to = block * side + lax.rem(place + k, side)
            copy_to(
                send_part.at[t - 1, :, rows_at(to, CAP), :], rows.at[:, my_slots, mine],
                a_send.at[t], half_recv.at[2 * t + turn], target * plane + to, q,
            )

        loop(0, plane, one)

    loop(1, 6, send_quarter)

    def turn_of(i):
        return i + 5 * lax.div(i + 1, 2)

    def fill_whole(i):
        at = rows_at(lax.rem(z + offset_of(turn_of(i)), 8), span)
        chosen = pick[at, :]
        send_all[i, 0] = product_of(chosen, normed[...]).astype(BF)
        send_all[i, 1] = (product_of(chosen, cot[...]) * weight[at, :]).astype(BF)

    loop(0, 3, fill_whole)
    own = rows_at(place, CAP)
    rows[0, my_slots, :] = send_all[0, 0, own, :]
    rows[1, my_slots, :] = send_all[0, 1, own, :]

    def send_whole(i):
        t = turn_of(i)
        target = lax.rem(z + offset_of(t), 8)

        def one(k):
            to = next_place(k)

            @pl.when(target * plane + to != me)
            def _():
                copy_to(
                    send_all.at[i, :, rows_at(to, CAP), :], rows.at[:, my_slots, :],
                    a_send.at[t], a_recv.at[t], target * plane + to, q,
                )

        loop(0, plane, one)


    send_whole(0)

    @pl.when(me > 0)
    def _():
        wait_for(extended.at[0:8], one_recv.at[0])

    copies[4].wait()
    now = (
        taps[0:1, :] * extended[8 : tokens + 8, :]
        + taps[1:2, :] * extended[7 : tokens + 7, :]
        + taps[2:3, :] * extended[6 : tokens + 6, :]
    )
    filtered[...] = now
    mixed[...] = (og[...].astype(F32) * now).astype(BF)
    chunk = min(256, width)

    def clear(m):
        cols = rows_at(m, chunk)
        gate_sum[cols, :] = jnp.zeros((chunk, part_of(gate_sum)), F32)
        up_sum[cols, :] = jnp.zeros((chunk, part_of(up_sum)), F32)
        down_sum[:, cols] = jnp.zeros((down_sum.shape[0], chunk), F32)

    loop(0, width // chunk, clear)
    for copy in copies[5:]:
        copy.wait()

    def add_grads(at):
        def one(m):
            cols = rows_at(m, chunk)
            here = rows[0, at, cols]
            gate_sum[cols, :] += rows_product(here, ggrad[at, :])
            up_sum[cols, :] += rows_product(here, ugrad[at, :])
            down_sum[:, cols] += rows_product(hidden[at, :], rows[1, at, cols])

        loop(0, width // chunk, one)

    def halves_at(t):
        source = source_at(t)
        return rows_at(2 * source, span // 2), rows_at(2 * source + 1, span // 2), source

    def pass_sum(t):
        upper, lower, source = halves_at(t)
        held_at = rows_at(source, span // 2)
        wait_for(far_in.at[0, held_at, :], far_left_recv.at[t])
        far_sum[0, held_at, :] = (partial[upper, of_right].astype(F32) + far_in[0, held_at, :].astype(F32)).astype(BF)
        copy_to(far_sum.at[0, held_at, :], summand.at[0, upper, :], rs_send.at[t], of_left_recv.at[t], me, right)
        wait_for(far_in.at[1, held_at, :], far_right_recv.at[t])
        far_sum[1, held_at, :] = (partial[lower, of_left].astype(F32) + far_in[1, held_at, :].astype(F32)).astype(BF)
        copy_to(far_sum.at[1, held_at, :], summand.at[1, lower, :], rs_send.at[t], of_right_recv.at[t], me, left)

    def pass_half(t, turn):
        block = lax.rem(lax.div(place, side) + turn, 2)
        piece = rows.at[:, rows_at(2 * source_at(t) + block, span // 2), mine]
        wait_for(piece, half_recv.at[2 * t + turn])
        copy_to(piece, piece, right_send.at[t], from_left.at[t], me, right)
        copy_to(piece, piece, left_send.at[t], from_right.at[t], me, left)

    def step(i):
        odd = lax.rem(i, 2)

        @pl.when(i < 6)
        def _():
            @pl.when(odd == 1)
            def _():
                pass_half(i, 0)

            @pl.when((odd == 1) & (i < 5))
            def _():
                pass_half(i + 1, 0)

            pass_half(i, 1)

        @pl.when(i == 3)
        def _():
            send_whole(1)
            send_whole(2)

        @pl.when((i >= 2) & (i < 7))
        def _():
            t = i - 1
            at = rows_at(source_at(t), span)
            wait_for(rows.at[:, at, of_left], from_left.at[t])
            half = rows.at[0, at, of_left]
            copy_to(half, half, fright_send.at[t], ffrom_left.at[t], me, right)
            wait_for(rows.at[:, at, of_right], from_right.at[t])
            half = rows.at[1, at, of_right]
            copy_to(half, half, fleft_send.at[t], ffrom_right.at[t], me, left)

        @pl.when((i >= 3) & (i < 8))
        def _():
            pass_sum(i - 3)

        @pl.when((i >= 2) & (i < 10))
        def _():
            t = i - 2
            at = rows_at(source_at(t), span)

            @pl.when((t >= 1) & (t < 6))
            def _():
                wait_for(rows.at[0, at, of_far], ffrom_left.at[t])
                wait_for(rows.at[1, at, of_far], ffrom_right.at[t])

            @pl.when(t == 0)
            def _():
                if plane > 1:
                    wait_for(rows.at[:, pl.ds(0, (plane - 1) * CAP), :], a_recv.at[0])

            @pl.when(t >= 6)
            def _():
                wait_for(rows.at[:, at, :], a_recv.at[t])

            here = rows[0, at, :]
            gate_pre = product_of(here, wg[...])
            up_pre = product_of(here, wu[...])
            hidden_grad = cols_product(rows[1, at, :], wd[...])
            sigmoid_gate = jax.nn.sigmoid(gate_pre)
            silu_gate = gate_pre * sigmoid_gate
            hidden[at, :] = (silu_gate * up_pre).astype(BF)
            gate_grad = (hidden_grad * up_pre * sigmoid_gate * (1.0 + gate_pre * (1.0 - sigmoid_gate))).astype(BF)
            up_grad = (hidden_grad * silu_gate).astype(BF)
            ggrad[at, :] = gate_grad
            ugrad[at, :] = up_grad
            partial[at, :] = (cols_product(gate_grad, wg[...]) + cols_product(up_grad, wu[...])).astype(BF)

            upper, lower, source = halves_at(t)
            held_at = rows_at(source, span // 2)
            copy_to(partial.at[upper, of_far], far_in.at[0, held_at, :], far_send.at[t], far_left_recv.at[t], me, right)
            copy_to(partial.at[lower, of_far], far_in.at[1, held_at, :], far_send.at[t], far_right_recv.at[t], me, left)
            copy_to(partial.at[lower, of_right], summand.at[0, lower, :], rs_send.at[t], of_left_recv.at[t], me, right)
            copy_to(partial.at[upper, of_left], summand.at[1, upper, :], rs_send.at[t], of_right_recv.at[t], me, left)

            @pl.when(t < 5)
            def _():
                add_grads(at)

        @pl.when((i >= 8) & (i < 11))
        def _():
            pass_sum(i - 3)

        @pl.when(i >= 4)
        def _():
            t = i - 4
            source = source_at(t)
            at = rows_at(source, span)
            wait_for(summand.at[0, at, :], of_left_recv.at[t])
            wait_for(summand.at[1, at, :], of_right_recv.at[t])
            added = partial[at, mine].astype(F32) + summand[0, at, :].astype(F32) + summand[1, at, :].astype(F32)
            total[at, :] = added.astype(BF)

            def one(k):
                to = source * plane + next_place(k)

                @pl.when(to != me)
                def _():
                    copy_to(total.at[rows_at(to, CAP), :], back.at[my_slots, :], one_send.at[1], one_recv.at[1], to, q)

            loop(0, plane, one)

    loop(1, 12, step)
    back[my_slots, :] = total[my_slots, :]

    def late_grads(t):
        add_grads(rows_at(source_at(t), span))

    loop(5, 7, late_grads)

    wait_for(back.at[pl.ds(0, (experts - 1) * CAP), :], one_recv.at[1])
    tok[:, mine] = rows_product(pick[...], back[...]).astype(BF)
    half = tokens // 2
    low, high = pl.ds(0, half), pl.ds(half, half)
    for h, at in ((0, low), (1, high)):
        copy_to(tok.at[at, mine], tok.at[at, mine], tright_send.at[h], tfrom_left.at[h], me, right)
    for h, at in ((1, high), (0, low)):
        copy_to(tok.at[at, mine], tok.at[at, mine], tleft_send.at[h], tfrom_right.at[h], me, left)
    loop(7, 8, late_grads)
    wait_for(tok.at[low, of_left], tfrom_left.at[0])
    copy_to(tok.at[low, of_left], tok.at[low, of_left], tf_send.at[0], tf_recv.at[0], me, right)
    wait_for(tok.at[high, of_right], tfrom_right.at[1])
    copy_to(tok.at[high, of_right], tok.at[high, of_right], tf_send.at[1], tf_recv.at[1], me, left)
    def narrow(m):
        cols = rows_at(m, chunk)
        gate_out[cols, :] = gate_sum[cols, :].astype(BF)
        up_out[cols, :] = up_sum[cols, :].astype(BF)
        down_out[:, cols] = down_sum[:, cols].astype(BF)

    loop(0, width // chunk, narrow)
    ready = (stream_out, og_out, ig_out, ci_out, ow_out, gate_out, up_out, down_out)
    finished = [pltpu.make_async_copy(a, b, out_sem.at[n]) for n, (a, b) in enumerate(zip(ready, outs))]
    for copy in finished[5:]:
        copy.start()

    wait_for(tok.at[high, of_left], tfrom_left.at[1])
    wait_for(tok.at[low, of_right], tfrom_right.at[0])
    wait_for(tok.at[low, of_far], tf_recv.at[0])
    wait_for(tok.at[high, of_far], tf_recv.at[1])

    def stream_rows(r):
        at = rows_at(r, 32)
        inv = inverse[at, :]
        unit = stream[at, :].astype(F32) * inv
        unit_grad = tok[at, :].astype(F32) * gain[...]
        along = jnp.mean(unit * unit_grad, axis=-1, keepdims=True)
        sgrad[at, :] = (cot[at, :].astype(F32) + inv * (unit_grad - unit * along)).astype(BF)

    loop(0, tokens // 32, stream_rows)

    block = width // experts
    pairs = experts // 2
    core = lax.rem(me, 2)
    here = lax.div(me, 2)
    groups = plane // 2
    cut = plane * block

    line = lax.rem(here, groups)

    def plane_of(j):
        half = lax.div(j + 1, 2)
        return lax.rem(z + 4 + half - 2 * half * lax.rem(j, 2), 8)

    def out_rows(j):
        at = plane_of(j)
        found = rows_product(sgrad[:, rows_at(at, cut)], mixed[...]).astype(BF)
        of_plane = rows_at(at, groups)
        owp[of_plane] = found.reshape(groups, 2, block, found.shape[-1])
        copy_to(owp.at[of_plane, 1 - core], pair.at[of_plane], pair_send.at[j], pair_recv.at[j], me + 1 - 2 * core, q)

    loop(0, 8, out_rows)

    def pair_sum(j):
        at = plane_of(j)
        of_plane = rows_at(at, groups)
        wait_for(pair.at[of_plane], pair_recv.at[j])
        psum[of_plane] = (owp[of_plane, core].astype(F32) + pair[of_plane].astype(F32)).astype(BF)

        def send_sum(k):
            to = lax.rem(line + k, groups)
            copy_to(
                psum.at[at * groups + to], row_in.at[k - 1, at], row_send, row_recv.at[j], 2 * (z * groups + to) + core, q
            )

        loop(1, groups, send_sum)

    loop(0, 8, pair_sum)

    mixed_grad = product_of(sgrad[...], ow[...])
    fgrad[0:tokens, :] = mixed_grad * og[...].astype(F32)

    @pl.when(me > 0)
    def _():
        copy_to(fgrad.at[0:8], fgrad.at[tokens : tokens + 8], one_send.at[3], one_recv.at[3], me - 1, q)

    @pl.when(me == experts - 1)
    def _():
        fgrad[tokens : tokens + 8, :] = jnp.zeros((8, part_of(fgrad)), F32)

    def row_sum(j):
        at = plane_of(j)
        found = psum[at * groups + line].astype(F32)
        if groups > 1:
            wait_for(row_in.at[:, at], row_recv.at[j])
            for k in range(groups - 1):
                found = found + row_in[k, at].astype(F32)
        row_total[at] = found.astype(BF)

        @pl.when(at != z)
        def _():
            copy_to(row_total.at[at], arrived.at[z], one_send.at[4], one_recv.at[4], 2 * (at * groups + line) + core, q)

    loop(0, 8, row_sum)
    arrived[z] = row_total[z]
    og_out[...] = (mixed_grad * filtered[...]).astype(BF)
    finished[1].start()
    stream_out[...] = sgrad[:, mine]
    finished[0].start()

    @pl.when(me < experts - 1)
    def _():
        wait_for(fgrad.at[tokens : tokens + 8], one_recv.at[3])

    product_grad = (
        taps[0:1, :] * fgrad[0:tokens, :] + taps[1:2, :] * fgrad[1 : tokens + 1, :] + taps[2:3, :] * fgrad[2 : tokens + 2, :]
    )
    ig_out[...] = (product_grad * ci[...].astype(F32)).astype(BF)
    ci_out[...] = (product_grad * ig[...].astype(F32)).astype(BF)
    finished[2].start()
    finished[3].start()

    def sent_rows(t):
        @pl.when((t >= 1) & (t < 6))
        def _():
            piece = rows.at[:, rows_at(0, span), mine]
            wait_for(piece, a_send.at[t])
            wait_for(piece, right_send.at[t])
            wait_for(piece, left_send.at[t])
            wait_for(rows.at[0, rows_at(0, span), mine], fright_send.at[t])
            wait_for(rows.at[0, rows_at(0, span), mine], fleft_send.at[t])

        @pl.when(t == 0)
        def _():
            if plane > 1:
                wait_for(rows.at[:, pl.ds(0, (plane - 1) * CAP), :], a_send.at[0])

        @pl.when(t >= 6)
        def _():
            wait_for(rows.at[:, rows_at(0, span), :], a_send.at[t])

        wait_for(summand.at[:, rows_at(0, span), :], rs_send.at[t])
        wait_for(summand.at[0, rows_at(0, span), :], far_send.at[t])

    loop(0, 8, sent_rows)
    wait_for(back.at[pl.ds(0, (experts - 1) * CAP), :], one_send.at[1])
    for h in range(2):
        wait_for(tok.at[low, mine], tright_send.at[h])
        wait_for(tok.at[low, mine], tleft_send.at[h])
        wait_for(tok.at[low, mine], tf_send.at[h])

    def pair_sent(j):
        wait_for(pair.at[pl.ds(0, groups)], pair_send.at[j])

    loop(0, 8, pair_sent)
    if groups > 1:
        wait_for(psum.at[pl.ds(0, 8 * (groups - 1))], row_send)

    @pl.when(me < experts - 1)
    def _():
        wait_for(extended.at[0:8], one_send.at[0])

    @pl.when(me > 0)
    def _():
        wait_for(fgrad.at[0:8], one_send.at[3])

    wait_for(arrived.at[pl.ds(0, 7)], one_recv.at[4])
    added = arrived[0].astype(F32)
    for p in range(1, 8):
        added = added + arrived[p].astype(F32)
    ow_out[...] = added
    finished[4].start()
    for copy in finished:
        copy.wait()
    wait_for(arrived.at[pl.ds(0, 7)], one_send.at[4])


def part_of(ref):
    return ref.shape[-1]


def whole_step(choice, scale, gain, taps, stream, cot, ig, ci, og, wg, wu, wd, ow, experts):
    tokens, width = cot.shape
    part = width // 4
    slots = experts * CAP
    plane = experts // 8
    hid = wg.shape[1]
    chan = og.shape[1]
    block = width // experts
    vm = pl.BlockSpec(memory_space=pltpu.VMEM)
    hbm = pl.BlockSpec(memory_space=pltpu.HBM)
    dma = pltpu.SemaphoreType.DMA
    return pl.pallas_call(
        functools.partial(step_kernel, plane),
        name="experts",
        out_shape=(
            jax.ShapeDtypeStruct((tokens, part), BF),
            jax.ShapeDtypeStruct((tokens, chan), BF),
            jax.ShapeDtypeStruct((tokens, chan), BF),
            jax.ShapeDtypeStruct((tokens, chan), BF),
            jax.ShapeDtypeStruct((block, chan), F32),
            jax.ShapeDtypeStruct((width, hid), BF),
            jax.ShapeDtypeStruct((width, hid), BF),
            jax.ShapeDtypeStruct((hid, width), BF),
        ),
        in_specs=[vm] * 4 + [hbm] * 9,
        out_specs=(hbm,) * 8,
        scratch_shapes=[
            pltpu.VMEM((tokens, width), BF),
            pltpu.VMEM((tokens, width), BF),
            pltpu.VMEM((tokens, chan), BF),
            pltpu.VMEM((tokens, chan), BF),
            pltpu.VMEM((tokens, chan), BF),
            pltpu.VMEM((width, hid), BF),
            pltpu.VMEM((width, hid), BF),
            pltpu.VMEM((hid, width), BF),
            pltpu.VMEM((width, chan), BF),
            pltpu.VMEM((tokens, 1), F32),
            pltpu.VMEM((tokens, width), BF),
            pltpu.VMEM((slots, tokens), BF),
            pltpu.VMEM((slots, 1), F32),
            pltpu.VMEM((3, 2, plane * CAP, width), BF),
            pltpu.VMEM((5, 2, plane * CAP, part), BF),
            pltpu.VMEM((2, slots, width), BF),
            pltpu.VMEM((slots, width), BF),
            pltpu.VMEM((2, slots, part), BF),
            pltpu.VMEM((2, slots // 2, part), BF),
            pltpu.VMEM((2, slots // 2, part), BF),
            pltpu.VMEM((slots, part), BF),
            pltpu.VMEM((slots, part), BF),
            pltpu.VMEM((slots, hid), BF),
            pltpu.VMEM((slots, hid), BF),
            pltpu.VMEM((slots, hid), BF),
            pltpu.VMEM((width, hid), BF),
            pltpu.VMEM((width, hid), BF),
            pltpu.VMEM((hid, width), BF),
            pltpu.VMEM((tokens, width), BF),
            pltpu.VMEM((tokens, width), BF),
            pltpu.VMEM((tokens + 8, chan), F32),
            pltpu.VMEM((tokens, chan), F32),
            pltpu.VMEM((tokens, chan), BF),
            pltpu.VMEM((tokens + 8, chan), F32),
            pltpu.VMEM((experts // 2, 2, block, chan), BF),
            pltpu.VMEM((experts // 2, block, chan), BF),
            pltpu.VMEM((experts // 2, block, chan), BF),
            pltpu.VMEM((max(1, plane // 2 - 1), 8, block, chan), BF),
            pltpu.VMEM((8, block, chan), BF),
            pltpu.VMEM((8, block, chan), BF),
            pltpu.VMEM((width, hid), F32),
            pltpu.VMEM((width, hid), F32),
            pltpu.VMEM((hid, width), F32),
            pltpu.VMEM((tokens, part), BF),
            pltpu.VMEM((tokens, chan), BF),
            pltpu.VMEM((tokens, chan), BF),
            pltpu.VMEM((tokens, chan), BF),
            pltpu.VMEM((block, chan), F32),
            dma((9,)),
            dma((8,)),
        ]
        + [dma((8,))] * 2
        + [dma((16,))]
        + [dma((8,))] * 14
        + [dma((2,))] * 6
        + [dma((5,))] * 2
        + [dma((8,))] * 2
        + [dma, dma((8,))],
        compiler_params=pltpu.CompilerParams(
            collective_id=0, has_side_effects=True, vmem_limit_bytes=62 * 1024 * 1024
        ),
    )(choice, scale, gain, taps, stream, cot, ig, ci, og, wg, wu, wd, ow)


def finish_kernel(pieces, *refs):
    given, outs, held, wide, in_sem, out_sem = refs[:8], refs[8:16], refs[16:24], refs[24:27], refs[27], refs[28]

    def cut(k):
        rows = given[k].shape[0] // pieces
        return [pl.ds(n * rows, rows) for n in range(pieces)] if k > 4 else [pl.ds(0, given[k].shape[0])]

    order = [(k, at) for k in (5, 6, 7, 0, 1, 2, 3, 4) for at in cut(k)]
    arriving = [pltpu.make_async_copy(given[k].at[at], held[k].at[at], in_sem.at[n]) for n, (k, at) in enumerate(order)]
    leaving = [
        pltpu.make_async_copy(wide[k - 5].at[at] if k > 4 else held[k].at[at], outs[k].at[at], out_sem.at[n])
        for n, (k, at) in enumerate(order)
    ]
    for copy in arriving:
        copy.start()
    for (k, at), copy, then in zip(order, arriving, leaving):
        copy.wait()
        if k > 4:
            wide[k - 5][at] = held[k][at].astype(F32)
        then.start()
    for copy in leaving:
        copy.wait()


def finished_outputs(arrays, pieces):
    types = [F32 if k > 3 else BF for k in range(len(arrays))]
    hbm = pl.BlockSpec(memory_space=pltpu.HBM)
    count = 5 + 3 * pieces
    return pl.pallas_call(
        functools.partial(finish_kernel, pieces),
        name="finish",
        out_shape=[jax.ShapeDtypeStruct(a.shape, t) for a, t in zip(arrays, types)],
        in_specs=[hbm] * 8,
        out_specs=[hbm] * 8,
        scratch_shapes=[pltpu.VMEM(a.shape, a.dtype) for a in arrays]
        + [pltpu.VMEM(a.shape, F32) for a in arrays[5:]]
        + [pltpu.SemaphoreType.DMA((count,)), pltpu.SemaphoreType.DMA((count,))],
        compiler_params=pltpu.CompilerParams(vmem_limit_bytes=60 * 1024 * 1024),
    )(*arrays)


def shards(
    cotangent,
    stream_in,
    norm_gain,
    out_gate,
    in_gate,
    conv_input,
    conv_taps,
    out_weight,
    expert_gate,
    expert_up,
    expert_down,
    expert_choice,
    route_scale,
):
    sp_size = lax.axis_size("sp")
    arrays = whole_step(
        expert_choice.T, route_scale.T, norm_gain[None], conv_taps, stream_in, cotangent, in_gate, conv_input, out_gate,
        expert_gate[0], expert_up[0], expert_down[0], out_weight, sp_size,
    )
    *others, grad_gate, grad_up, grad_down = finished_outputs(arrays, 4)
    return (*others, grad_gate[None], grad_up[None], grad_down[None])


def solution(mesh):
    placed = (
        P("sp", None),
        P("sp", None),
        P(),
        P("sp", "tp"),
        P("sp", "tp"),
        P("sp", "tp"),
        P(None, "tp"),
        P(None, "tp"),
        P("sp", None, "tp"),
        P("sp", None, "tp"),
        P("sp", "tp", None),
        P("sp", None),
        P("sp", None),
    )
    return jax.shard_map(
        shards,
        mesh=mesh,
        in_specs=placed,
        out_specs=(
            P("sp", "tp"),
            P("sp", "tp"),
            P("sp", "tp"),
            P("sp", "tp"),
            P("sp", "tp"),
            P("sp", None, "tp"),
            P("sp", None, "tp"),
            P("sp", "tp", None),
        ),
        check_vma=False,
    )
```
